32 devices in a mesh: fs: 16 (over z, y, x), tp: 2 (over core).
Axes of the slice: x: 2, y: 2, z: 4, core: 2. Of those that a mesh axis runs over, the one named last changes fastest.
Arguments:
- tokens: bfloat16 [6144, 2048], P('fs', 'tp'), may hold values from -24 to 24, as said below
- mixer_gain: float32 [2048], replicated, may hold values from 0.1 to 1.9
- w_content: float32 [2048, 1024], P('fs', 'tp'), may hold values from -0.125 to 0.125
- w_spatial: float32 [2048, 1024], P('fs', 'tp'), may hold values from -0.125 to 0.125
- content_scale: float32 [1024], P('tp'), may hold values from 0.5 to 2
- spatial_scale: float32 [1024], P('tp'), may hold values from 0.2 to 3.5, as said below
- spatial_gain: float32 [1024], P('tp'), may hold values from 0.1 to 1.9
- block_mixing: bfloat16 [8, 128, 128], P('tp'), may hold values from -0.5 to 0.5
- block_bias: float32 [8, 128], P('tp'), may hold values from -6 to 6
- w_project: float32 [1024, 2048], P('tp', 'fs'), may hold values from -0.1875 to 0.1875
- project_scale: float32 [2048], P('fs'), may hold values from 0.5 to 2
- channel_gain: float32 [2048], replicated, may hold values from 0.1 to 1.9
- w_up: float32 [2048, 8192], P('fs', 'tp'), may hold values from -0.125 to 0.125
- up_scale: float32 [8192], P('tp'), may hold values from 0.5 to 2
- w_down: float32 [8192, 2048], P('tp', 'fs'), may hold values from -0.0625 to 0.0625
- down_scale: float32 [2048], P('fs'), may hold values from 0.5 to 2
Outputs:
- layer_out: bfloat16 [6144, 2048], P('fs', 'tp')
The draws below stay inside these ranges and needn't reach their ends.
Inputs may be any that keep to these rules, and one draw needn't show every extreme that they name: `tokens`: activations whose features and rows have differing scales. `spatial_scale`: positive column scales.
All inputs are finite; a program needn't handle non-finite values.
Results may differ from the reference program's by a relative error of at most 0.019.
Values may be sent and summed in bfloat16 or wider, within the bound.
A program may use at most 128 MiB of HBM per device.

```python
import math
import jax
import jax.numpy as jnp
from jax import lax

D = 2048
GROUPS = 8
GCH = 128
W_SGU = 1024
FF = 8192
BLOCK = 128
TOK_DEV = 384
TOKENS = 6144
N_FS = 16
N_TP = 2


def draw_tokens(key, part):
    first_key = jax.random.fold_in(key, 11)
    second_key = jax.random.fold_in(key, 12)
    third_key = jax.random.fold_in(key, 13)
    column_scales = jnp.exp(jax.random.uniform(second_key, (D,), jnp.float32, math.log(0.3), math.log(3.0)))
    base_values = jax.random.truncated_normal(first_key, -4.0, 4.0, (TOKENS, D), jnp.float32)
    row_scales = jnp.exp(jax.random.uniform(third_key, (TOKENS, 1), jnp.float32, math.log(0.5), math.log(2.0)))
    return (base_values * column_scales[None, :] * row_scales).astype(jnp.bfloat16)


def draw_spatial_scale(key, part):
    jitter_key = jax.random.fold_in(key, 21)
    position = jnp.arange(W_SGU).astype(jnp.float32) / (W_SGU - 1)
    jitter = jnp.exp(jax.random.uniform(jitter_key, (W_SGU,), jnp.float32, -0.35, 0.35))
    base_scale = jnp.exp(math.log(0.5) + (math.log(1.6) - math.log(0.5)) * position)
    return (base_scale * jitter).astype(jnp.float32)


def shard_levels(own_key, dims, shards, smallest, largest):
    factor_of = 1.0
    for dim, blocks in shards:
        heights = jax.random.uniform(jax.random.fold_in(jax.random.fold_in(own_key, 6), dim), (blocks,), jnp.float32, smallest / len(shards), largest / len(shards))
        factor_of = factor_of * jnp.repeat(jnp.exp(heights), dims[dim] // blocks).reshape((-1,) + (1,) * (len(dims) - 1 - dim))
    return factor_of


def scatter_about(stream_key, dims, scale, reach, split=(), kind=jnp.bfloat16):
    values = scale * jax.random.normal(stream_key, dims, jnp.float32)
    if split:
        values = values * shard_levels(stream_key, dims, split, -0.22, 0.18)
    return jnp.clip(values, -reach, reach).astype(kind)


def setup_inputs(seed: int = 0) -> dict:
    seeds = jax.random.split(jax.random.key(seed), 17)
    return {
        "tokens": draw_tokens(jax.random.fold_in(seeds[16], 71), 0),
        "mixer_gain": jnp.clip(1.0 + 0.18 * jax.random.normal(seeds[1], (D,), jnp.float32), 0.1, 1.9),
        "w_content": scatter_about(seeds[2], (D, W_SGU), D ** -0.5, 0.125, ((0, 16), (1, 2)), jnp.float32),
        "w_spatial": scatter_about(seeds[3], (D, W_SGU), D ** -0.5, 0.125, ((0, 16), (1, 2)), jnp.float32),
        "content_scale": jnp.clip(jnp.exp(math.log(2.0) - 1.3862944 * jax.random.uniform(seeds[4], (W_SGU,), jnp.float32) ** shard_levels(seeds[4], (W_SGU,), ((0, 2),), -0.2, 0.2)), 0.5, 2.0),
        "spatial_scale": draw_spatial_scale(jax.random.fold_in(seeds[16], 71), 0),
        "spatial_gain": jnp.clip(1.0 + 0.18 * jax.random.normal(seeds[6], (W_SGU,), jnp.float32), 0.1, 1.9),
        "block_mixing": scatter_about(seeds[7], (GROUPS, BLOCK, BLOCK), BLOCK ** -0.5, 0.5, ((0, 2),)),
        "block_bias": scatter_about(seeds[8], (GROUPS, BLOCK), 1.0, 6.0, ((0, 2),), jnp.float32),
        "w_project": scatter_about(seeds[9], (W_SGU, D), W_SGU ** -0.5, 0.1875, ((0, 2), (1, 16)), jnp.float32),
        "project_scale": jnp.clip(jnp.exp(math.log(2.0) - 1.3862944 * jax.random.uniform(seeds[10], (D,), jnp.float32) ** shard_levels(seeds[10], (D,), ((0, 16),), -0.2, 0.2)), 0.5, 2.0),
        "channel_gain": jnp.clip(1.0 + 0.18 * jax.random.normal(seeds[11], (D,), jnp.float32), 0.1, 1.9),
        "w_up": scatter_about(seeds[12], (D, FF), D ** -0.5, 0.125, ((0, 16), (1, 2)), jnp.float32),
        "up_scale": jnp.clip(jnp.exp(math.log(2.0) - 1.3862944 * jax.random.uniform(seeds[13], (FF,), jnp.float32) ** shard_levels(seeds[13], (FF,), ((0, 2),), -0.2, 0.2)), 0.5, 2.0),
        "w_down": scatter_about(seeds[14], (FF, D), FF ** -0.5, 0.0625, ((0, 2), (1, 16)), jnp.float32),
        "down_scale": jnp.clip(jnp.exp(math.log(2.0) - 1.3862944 * jax.random.uniform(seeds[15], (D,), jnp.float32) ** shard_levels(seeds[15], (D,), ((0, 16),), -0.2, 0.2)), 0.5, 2.0),
    }


EPSILON = 1e-06

def normalize_rows(token_rows, gain_vector):
    values = token_rows.astype(jnp.float32)
    scaled = values * lax.rsqrt(lax.optimization_barrier(jnp.mean(values * values, axis=-1, keepdims=True)) + EPSILON)
    return (scaled * gain_vector).astype(jnp.bfloat16)

def split_sum(left, right, column_scale, shard_count):
    shard_width = left.shape[1] // shard_count
    running = jnp.zeros((left.shape[0], right.shape[1]), jnp.float32)
    for shard_index in range(shard_count):
        low = shard_index * shard_width
        partial_value = jnp.dot(left[:, low:low + shard_width], right[low:low + shard_width, :], preferred_element_type=jnp.float32) * column_scale
        rounded = lax.optimization_barrier(partial_value.astype(jnp.bfloat16))
        running = running + rounded.astype(jnp.float32)
    return running

def reference(tokens, mixer_gain, w_content, w_spatial, content_scale, spatial_scale, spatial_gain, block_mixing, block_bias, w_project, project_scale, channel_gain, w_up, up_scale, w_down, down_scale):
    content_weight = w_content.astype(jnp.bfloat16)
    spatial_weight = w_spatial.astype(jnp.bfloat16)
    project_weight = w_project.astype(jnp.bfloat16)
    up_weight = w_up.astype(jnp.bfloat16)
    down_weight = w_down.astype(jnp.bfloat16)
    causal_mask = jnp.tril(jnp.ones((BLOCK, BLOCK), dtype=bool))
    mixing_weights = jnp.where(causal_mask[None, :, :], block_mixing.astype(jnp.float32), jnp.float32(0.0))

    def one_sequence(token_rows):
        normed = normalize_rows(token_rows, mixer_gain)
        content = jax.nn.gelu(jnp.dot(normed, content_weight, preferred_element_type=jnp.float32) * content_scale)
        spatial = jax.nn.gelu(jnp.dot(normed, spatial_weight, preferred_element_type=jnp.float32) * spatial_scale)
        spatial_norm = (spatial * lax.rsqrt(lax.optimization_barrier(jnp.mean(spatial * spatial, axis=-1, keepdims=True)) + EPSILON) * spatial_gain).astype(jnp.bfloat16)
        grouped = spatial_norm.astype(jnp.float32).reshape(TOK_DEV // BLOCK, BLOCK, GROUPS, GCH)
        mixed_block = jnp.einsum('gts,nsgc->ntgc', mixing_weights, grouped) + block_bias.T[None, :, :, None]
        gated = (content * mixed_block.reshape(TOK_DEV, W_SGU)).astype(jnp.bfloat16)
        mixer_sum = split_sum(gated, project_weight, project_scale, N_TP)
        middle = (token_rows.astype(jnp.float32) + mixer_sum).astype(jnp.bfloat16)
        channel_normed = normalize_rows(middle, channel_gain)
        up_linear = jnp.dot(channel_normed, up_weight, preferred_element_type=jnp.float32) * up_scale
        hidden = jnp.square(jax.nn.relu(up_linear)).astype(jnp.bfloat16)
        channel_sum = split_sum(hidden, down_weight, down_scale, N_TP)
        return (middle.astype(jnp.float32) + channel_sum).astype(jnp.bfloat16)
    layer_out = lax.map(one_sequence, tokens.reshape(N_FS, TOK_DEV, D))
    return layer_out.reshape(TOKENS, D)
```

```python
import functools

import jax
import jax.numpy as jnp
from jax import lax
from jax.experimental import pallas as pl
from jax.experimental.pallas import tpu as pltpu
from jax.sharding import PartitionSpec as P

EPSILON = 1e-06


def normalize_rows(token_rows, gain_vector):
    values = token_rows.astype(jnp.float32)
    scaled = values * lax.rsqrt(jnp.mean(values * values, axis=-1, keepdims=True) + EPSILON)
    return (scaled * gain_vector).astype(jnp.bfloat16)


def shards(
    tokens,
    mixer_gain,
    w_content,
    w_spatial,
    content_scale,
    spatial_scale,
    spatial_gain,
    block_mixing,
    block_bias,
    w_project,
    project_scale,
    channel_gain,
    w_up,
    up_scale,
    w_down,
    down_scale,
):
    content_weight = w_content.astype(jnp.bfloat16)
    spatial_weight = w_spatial.astype(jnp.bfloat16)
    project_weight = w_project.astype(jnp.bfloat16)
    up_weight = w_up.astype(jnp.bfloat16)
    down_weight = w_down.astype(jnp.bfloat16)
    project_full, down_full = (
        lax.all_gather(project_scale, "fs", axis=0, tiled=True),
        lax.all_gather(down_scale, "fs", axis=0, tiled=True),
    )
    gathered_rows = lax.all_gather(tokens, "tp", axis=1, tiled=True)
    normed = normalize_rows(gathered_rows, mixer_gain)
    row_count = gathered_rows.shape[0]
    content_full, spatial_full, project_cols = (
        lax.all_gather(content_weight, "fs", axis=0, tiled=True),
        lax.all_gather(spatial_weight, "fs", axis=0, tiled=True),
        lax.all_gather(project_weight, "fs", axis=1, tiled=True),
    )
    content_linear = jnp.dot(normed, content_full, preferred_element_type=jnp.float32)
    spatial_linear = jnp.dot(normed, spatial_full, preferred_element_type=jnp.float32)
    content = jax.nn.gelu(content_linear * content_scale)
    spatial = jax.nn.gelu(spatial_linear * spatial_scale)
    square_sums = lax.psum(jnp.sum(spatial * spatial, axis=1), "tp")
    total_width = spatial.shape[1] * lax.axis_size("tp")
    spatial_norm = (
        spatial * lax.rsqrt(square_sums / total_width + EPSILON)[:, None] * spatial_gain
    ).astype(jnp.bfloat16)
    groups_here = block_mixing.shape[0]
    block_size = block_mixing.shape[1]
    group_width = spatial_norm.shape[1] // groups_here
    causal_mask = jnp.tril(jnp.ones((block_size, block_size), dtype=bool))
    mixing_weights = jnp.where(causal_mask[None, :, :], block_mixing, jnp.zeros_like(block_mixing))
    grouped = spatial_norm.reshape(row_count // block_size, block_size, groups_here, group_width)
    mixed_block = (
        jnp.einsum("gts,nsgc->ntgc", mixing_weights, grouped, preferred_element_type=jnp.float32)
        + block_bias.T[None, :, :, None]
    )
    gated = (content * mixed_block.reshape(row_count, spatial_norm.shape[1])).astype(jnp.bfloat16)
    mixer_terms = jnp.dot(gated, project_cols, preferred_element_type=jnp.float32) * project_full
    mixer_sum = lax.psum_scatter(
        mixer_terms.astype(jnp.bfloat16), "tp", scatter_dimension=1, tiled=True
    ).astype(jnp.float32)
    middle = (tokens.astype(jnp.float32) + mixer_sum).astype(jnp.bfloat16)
    middle_rows = lax.all_gather(middle, "tp", axis=1, tiled=True)
    channel_normed = normalize_rows(middle_rows, channel_gain)
    up_full, down_cols = (
        lax.all_gather(up_weight, "fs", axis=0, tiled=True),
        lax.all_gather(down_weight, "fs", axis=1, tiled=True),
    )
    up_linear = jnp.dot(channel_normed, up_full, preferred_element_type=jnp.float32)
    hidden = jnp.square(jax.nn.relu(up_linear * up_scale)).astype(jnp.bfloat16)
    channel_terms = jnp.dot(hidden, down_cols, preferred_element_type=jnp.float32) * down_full
    channel_sum = lax.psum_scatter(
        channel_terms.astype(jnp.bfloat16), "tp", scatter_dimension=1, tiled=True
    ).astype(jnp.float32)
    return (middle.astype(jnp.float32) + channel_sum).astype(jnp.bfloat16)


LINES = 4
PLANE = 4
MESH = pl.DeviceIdType.MESH


def layer_kernel(
    sizes,
    tokens_ref,
    mixer_gain_ref,
    content_ref,
    spatial_ref,
    content_scale_ref,
    spatial_scale_ref,
    spatial_gain_ref,
    mixing_ref,
    bias_ref,
    project_ref,
    project_scale_ref,
    channel_gain_ref,
    up_hbm,
    up_scale_ref,
    down_hbm,
    down_scale_ref,
    out_ref,
    up_ref,
    down_ref,
    load_sem,
    token_rows,
    normed,
    gate_weights,
    project_full,
    gate_other,
    project_other,
    up_own,
    down_own,
    up_full,
    down_full,
    content_buf,
    spatial_buf,
    gated,
    sums,
    sums_in,
    part,
    part_in,
    share,
    share_in,
    middle,
    rows_all,
    hidden,
    terms,
    terms_in,
    cross_in,
    line_in,
    token_send,
    token_recv,
    half_send,
    half_recv,
    gate_line_send,
    gate_line_recv,
    gate_send,
    gate_recv,
    swap_send,
    swap_recv,
    across_send,
    across_recv,
    beside_send,
    beside_recv,
    sum_send,
    sum_recv,
    part_send,
    part_recv,
    share_send,
    share_recv,
    middle_send,
    middle_recv,
    row_send,
    row_recv,
    fwd_send,
    fwd_recv,
    term_send,
    term_recv,
    cross_send,
    cross_recv,
    line_send,
    line_recv,
):
    rows, half = tokens_ref.shape
    width = 2 * half
    depth = content_ref.shape[0]
    channels = content_ref.shape[1]
    share_width = channels // 2
    units = up_full.shape[1]
    slab = 2 * depth
    fine = sizes["fine"]
    tile = sizes["tile"]
    groups, block_size = mixing_ref.shape[0], mixing_ref.shape[1]
    blocks = rows // block_size
    steps = rows // block_size
    me = lax.axis_index("fs")
    core = lax.axis_index("tp")
    z = me // PLANE
    p = me % PLANE
    y = p // 2
    x = p % 2
    zh = z // 2
    zl = z % 2
    other = 1 - core
    f32, bf16 = jnp.float32, jnp.bfloat16

    def span(start, size, by=128):
        return pl.ds(pl.multiple_of(start, by), size)

    beside_x = me + 1 - 2 * x
    beside_y = me + 2 - 4 * y
    beside_z = me + PLANE * (1 - 2 * zl)
    corner = beside_z + 1 - 2 * x
    far_z = me + 2 * PLANE * (1 - 2 * zh)
    inner = (z > 0) & (z < LINES - 1)
    pair = {"tp": other}
    mine = span(core * half, half)

    def remote(src, dst, send, recv, where):
        return pltpu.make_async_remote_copy(
            src_ref=src, dst_ref=dst, send_sem=send, recv_sem=recv, device_id=where, device_id_type=MESH
        )

    loads = [
        pltpu.make_async_copy(up_hbm, up_ref, load_sem.at[0]),
        pltpu.make_async_copy(down_hbm, down_ref, load_sem.at[1]),
    ]
    for load in loads:
        load.start()
    barrier = pltpu.get_barrier_semaphore()
    friends = [{"fs": i} for i in (beside_x, beside_y, beside_z, corner, far_z)]
    friends += [pair, {"fs": beside_x, "tp": other}]
    for friend in friends:
        pl.semaphore_signal(barrier, inc=1, device_id=friend, device_id_type=MESH)

    @pl.when(inner)
    def _():
        pl.semaphore_signal(
            barrier, inc=1, device_id={"fs": me + PLANE * (2 * zl - 1)}, device_id_type=MESH
        )

    own_channels = span(x * share_width, share_width)
    own_depth = span(me * depth, depth)

    def halves(channel_half, weights, project):
        at = span(channel_half * share_width, share_width)
        weights[:, pl.ds(0, share_width)] = content_ref[:, at].astype(bf16)
        weights[:, pl.ds(share_width, share_width)] = spatial_ref[:, at].astype(bf16)
        project[...] = (project_ref[at, :] * project_scale_ref[...]).astype(bf16)

    halves(1 - x, gate_other, project_other)
    halves(x, gate_weights.at[own_depth, :], project_full.at[:, own_depth])
    token_rows[0, :, mine] = tokens_ref[...]
    pl.semaphore_wait(barrier, len(friends) + inner.astype(jnp.int32))

    def slab_at(q, yy):
        return span((q * PLANE + yy * 2) * depth, slab)

    def gate_refs(q, yy):
        at = slab_at(q, yy)
        return gate_weights.at[at, :], project_full.at[:, at]

    def gate_line(q, side, step):
        refs = gate_refs(q, y)
        return [
            remote(
                refs[a], refs[a], gate_line_send.at[a, side, q], gate_line_recv.at[a, q],
                {"fs": me + step * PLANE},
            )
            for a in range(2)
        ]

    def gate_cross(q, yy):
        refs = gate_refs(q, yy)
        return [
            remote(refs[a], refs[a], gate_send.at[a, q], gate_recv.at[a, q], {"fs": beside_y}) for a in range(2)
        ]

    half_copies = [
        remote(gate_other, gate_weights.at[own_depth, :], half_send.at[0], half_recv.at[0], {"fs": beside_x}),
        remote(project_other, project_full.at[:, own_depth], half_send.at[1], half_recv.at[1], {"fs": beside_x}),
    ]

    swap_to = (beside_x, beside_z, corner)
    swap_part = (2 * zl + 1 - x, 2 * (1 - zl) + x, 2 * (1 - zl) + 1 - x)

    def swap(a, k):
        theirs = span(swap_part[k] * units, units)
        src = up_own.at[:, theirs] if a == 0 else down_own.at[theirs, :]
        dst = up_full.at[own_depth, :] if a == 0 else down_full.at[:, own_depth]
        return remote(src, dst, swap_send.at[a, k], swap_recv.at[a, k], {"fs": swap_to[k]})

    def ff_ref(a, q, yy):
        return up_full.at[slab_at(q, yy), :] if a == 0 else down_full.at[:, slab_at(q, yy)]

    def line_of(g, b):
        return 2 * (zh if g == 0 else 1 - zh) + b

    def across(a, b):
        ref = ff_ref(a, line_of(0, b), y)
        return remote(ref, ref, across_send.at[a, b], across_recv.at[a, b], {"fs": far_z})

    def beside(a, g, b):
        ref = ff_ref(a, line_of(g, b), y)
        return remote(ref, ref, beside_send.at[a, g, b], beside_recv.at[a, g, b], {"fs": beside_y})

    def relay_gate(d):
        for side, step in ((0, 1), (1, -1)):
            q = z - step * d

            @pl.when((q >= 0) & (q < LINES))
            def _(q=q, side=side, step=step):
                for copy in gate_line(q, side, step):
                    copy.wait_recv()

                @pl.when((z + step >= 0) & (z + step < LINES))
                def _():
                    for copy in gate_line(q, side, step):
                        copy.start()

                for copy in gate_cross(q, y):
                    copy.start()

    for copy in half_copies:
        copy.start()
    token_pair = remote(tokens_ref, token_rows.at[0, :, mine], token_send.at[0], token_recv.at[0], pair)
    token_pair.start()
    for load in loads:
        load.wait()

    @pl.loop(0, up_own.shape[1] // units)
    def _(j):
        up_own[:, span(j * units, units)] = up_ref[:, span(j * units, units)].astype(bf16)

    quarter = span((2 * zl + x) * units, units)
    swap(0, 0).start()
    token_cross = remote(
        tokens_ref, token_rows.at[1, :, mine], token_send.at[1], token_recv.at[1], {"fs": beside_x}
    )
    token_cross.start()
    up_full[own_depth, :] = up_ref[:, quarter].astype(bf16)

    @pl.loop(0, up_own.shape[1] // units)
    def _(j):
        down_own[span(j * units, units), :] = (
            down_ref[span(j * units, units), :] * down_scale_ref[...]
        ).astype(bf16)

    down_full[:, own_depth] = (down_ref[quarter, :] * down_scale_ref[...]).astype(bf16)

    for copy in half_copies:
        copy.wait_recv()
    for side, step in ((0, 1), (1, -1)):

        @pl.when((z + step >= 0) & (z + step < LINES))
        def _(side=side, step=step):
            for copy in gate_line(z, side, step):
                copy.start()

    for copy in gate_cross(z, y):
        copy.start()
    swap(0, 1).start()
    swap(0, 2).start()

    def normalize(source, gain_ref, target, first, count):
        @pl.loop(0, count // fine)
        def _(i):
            these = span(first + i * fine, fine, fine)
            values = source[these, :].astype(f32)
            scaled = values * lax.rsqrt(jnp.mean(values * values, axis=-1, keepdims=True) + EPSILON)
            target[these, :] = (scaled * gain_ref[...]).astype(bf16)

    token_pair.wait()
    normalize(token_rows.at[0], mixer_gain_ref, normed.at[0], 0, rows)
    relay_gate(1)
    relay_gate(2)
    for k in range(3):
        swap(1, k).start()
    for k in range(3):
        swap(0, k).wait_recv()
    for b in range(2):
        across(0, b).start()
    relay_gate(3)
    for b in range(2):
        beside(0, 0, b).start()

    token_cross.wait()
    token_forward = remote(
        token_rows.at[1, :, mine], token_rows.at[1, :, mine], token_send.at[2], token_recv.at[2], pair
    )
    token_forward.start()
    token_forward.wait()
    normalize(token_rows.at[1], mixer_gain_ref, normed.at[1], 0, rows)

    for q in range(LINES):
        for copy in gate_cross(q, 1 - y):
            copy.wait_recv()

    @pl.loop(0, 2)
    def _(s):
        linear = jnp.dot(normed[s], gate_weights[:, pl.ds(share_width, share_width)], preferred_element_type=f32)
        spatial_buf[s] = jax.nn.gelu(linear * spatial_scale_ref[:, own_channels])

    sums[...] = jnp.zeros_like(sums)
    for s in range(2):
        for n in range(blocks):
            values = spatial_buf[s, pl.ds(n * block_size, block_size), :]
            total = jnp.sum(values * values, axis=1, keepdims=True)
            sums[pl.ds(s * blocks + n, 1), :] = jnp.broadcast_to(total, (block_size, block_size)).T[:1, :]
    sum_to = (pair, {"fs": beside_x}, {"fs": beside_x, "tp": other})
    sum_copies = [remote(sums, sums_in.at[k], sum_send.at[k], sum_recv.at[k], sum_to[k]) for k in range(3)]
    for copy in sum_copies:
        copy.start()

    @pl.loop(0, 2)
    def _(s):
        linear = jnp.dot(normed[s], gate_weights[:, pl.ds(0, share_width)], preferred_element_type=f32)
        content_buf[s] = jax.nn.gelu(linear * content_scale_ref[:, own_channels])

    for copy in sum_copies:
        copy.wait_recv()

    causal = lax.broadcasted_iota(jnp.int32, (block_size, block_size), 0) >= lax.broadcasted_iota(
        jnp.int32, (block_size, block_size), 1
    )
    own_groups = groups // 2
    group_width = channels // groups
    part_copies = [
        remote(
            part.at[s, :, span(other * half, half)], part_in.at[s], part_send.at[s], part_recv.at[s], pair
        )
        for s in range(2)
    ]
    for s in (1, 0):
        for n in range(blocks):
            these = pl.ds(n * block_size, block_size)
            here, there = pl.ds(s * blocks + n, 1), pl.ds((1 - s) * blocks + n, 1)
            total = (sums[here, :] + sums_in[0, here, :]) + (sums_in[1, there, :] + sums_in[2, there, :])
            scale = lax.rsqrt(total / (2 * channels) + EPSILON)
            scale = jnp.broadcast_to(scale, (block_size, block_size)).T[:, :1]
            for g in range(own_groups):
                group = x * own_groups + g
                weights = jnp.where(causal, mixing_ref[group].astype(f32), 0.0).astype(bf16)
                bias = jnp.broadcast_to(bias_ref[pl.ds(group, 1), :], (block_size, block_size)).T[:, :1]
                at = pl.ds(g * group_width, group_width)
                gain = spatial_gain_ref[:, span(group * group_width, group_width)]
                spatial_norm = (spatial_buf[s, these, at] * scale * gain).astype(bf16)
                mixed = jnp.dot(weights, spatial_norm, preferred_element_type=f32) + bias
                gated[s, these, at] = (content_buf[s, these, at] * mixed).astype(bf16)

        @pl.loop(0, width // (2 * tile))
        def _(j, s=s):
            at = span(j * 2 * tile, 2 * tile)
            part[s, :, at] = jnp.dot(gated[s], project_full[:, at], preferred_element_type=f32).astype(bf16)

        part_copies[s].start()

    def step_rows(i):
        return pl.ds(i * block_size, block_size)

    share_copies = [
        remote(
            share.at[step_rows(i), :], share_in.at[step_rows(i), :], share_send.at[i], share_recv.at[i],
            {"fs": beside_x},
        )
        for i in range(steps)
    ]
    part_copies[1].wait_recv()
    for i in range(steps):
        these = step_rows(i)
        share[these, :] = (part[1, these, mine].astype(f32) + part_in[1, these, :].astype(f32)).astype(bf16)
        share_copies[i].start()
    part_copies[0].wait_recv()

    for k in range(3):
        swap(1, k).wait_recv()
    for b in range(2):
        across(1, b).start()
    across(0, 0).wait_recv()
    beside(0, 1, 0).start()
    beside(1, 0, 0).start()

    middle_copies = [
        remote(
            middle.at[step_rows(i), mine], middle.at[step_rows(i), mine], middle_send.at[i], middle_recv.at[i], pair
        )
        for i in range(steps)
    ]

    def row_copy(k, i):
        src = rows_all.at[2 if k == 2 else 0, step_rows(i), mine]
        dst = rows_all.at[k + 1, step_rows(i), mine]
        return remote(src, dst, row_send.at[k, i], row_recv.at[k, i], {"fs": beside_z if k == 1 else beside_x})

    def forward(k, i):
        ref = rows_all.at[k + 1, step_rows(i), mine]
        return remote(ref, ref, fwd_send.at[k, i], fwd_recv.at[k, i], pair)

    for i in range(steps):
        these = step_rows(i)
        share_copies[i].wait_recv()
        total = part[0, these, mine].astype(f32) + part_in[0, these, :].astype(f32)
        total = total + share_in[these, :].astype(f32)
        middle[these, mine] = (tokens_ref[these, :].astype(f32) + total).astype(bf16)
        middle_copies[i].start()
        middle_copies[i].wait_recv()
        normalize(middle, channel_gain_ref, rows_all.at[0], i * block_size, block_size)
        row_copy(1, i).start()
        row_copy(0, i).start()

    across(0, 1).wait_recv()
    beside(0, 1, 1).start()
    beside(1, 0, 1).start()
    for i in range(steps):
        row_copy(1, i).wait_recv()
        row_copy(2, i).start()
        forward(1, i).start()
        row_copy(0, i).wait_recv()
        forward(0, i).start()
    across(1, 0).wait_recv()
    beside(1, 1, 0).start()
    for g in range(2):
        for b in range(2):
            beside(0, g, b).wait_recv()

    up_tile = sizes["up_tile"]
    unit_base = (2 * zl + x) * units

    def up_product(r):
        @pl.loop(0, units // up_tile)
        def _(j):
            at = span(j * up_tile, up_tile)
            linear = jnp.dot(rows_all[r], up_full[:, at], preferred_element_type=f32)
            linear = linear * up_scale_ref[:, span(unit_base + j * up_tile, up_tile)]
            hidden[r, :, at] = jnp.square(jnp.maximum(linear, 0.0)).astype(bf16)

    up_product(0)
    for k in range(2):
        for i in range(steps):
            forward(k, i).wait_recv()
        up_product(k + 1)
    for i in range(steps):
        row_copy(2, i).wait_recv()
        forward(2, i).start()
    for i in range(steps):
        forward(2, i).wait_recv()
    up_product(3)

    pieces = [(g, b, same) for g in range(2) for same in range(2) for b in range(2)]

    def owner(i):
        return (zh if pieces[i][0] == 0 else 1 - zh) == core

    def term_copy(i):
        return remote(terms.at[i], terms_in.at[i % 4], term_send.at[i % 4], term_recv.at[i % 4], pair)

    def cross_copy(i, k):
        return remote(
            terms.at[i, 2 * k + 1], cross_in.at[i % 4, k], cross_send.at[i % 4, k], cross_recv.at[i % 4, k],
            {"fs": beside_x},
        )

    def line_copy(i):
        return remote(
            terms.at[i, 2], line_in.at[i % 4], line_send.at[i % 4], line_recv.at[i % 4], {"fs": beside_z}
        )

    def columns(i):
        g, b, same = pieces[i]
        yy = y if same == 0 else 1 - y
        return line_of(g, b), yy

    def term_step(i):
        g, b, same = pieces[i]
        if same == 1:
            beside(1, g, b).wait_recv()
        q, yy = columns(i)

        @pl.loop(0, 4)
        def _(r):
            terms[i, r] = jnp.dot(hidden[r], down_full[:, slab_at(q, yy)], preferred_element_type=f32).astype(bf16)

        @pl.when(jnp.logical_not(owner(i)))
        def _():
            term_copy(i).start()

        @pl.when(owner(i))
        def _():
            term_copy(i).wait_recv()

            def add(r):
                @pl.loop(0, rows // fine)
                def _(c):
                    these = span(c * fine, fine, fine)
                    terms[i, r, these, :] = (
                        terms[i, r, these, :].astype(f32) + terms_in[i % 4, r, these, :].astype(f32)
                    ).astype(bf16)

            for r in (3, 1):
                add(r)
                cross_copy(i, r // 2).start()
            for r in (2, 0):
                add(r)

    def cross_step(i):
        @pl.when(owner(i))
        def _():
            cross_copy(i, 1).wait_recv()

            @pl.loop(0, rows // fine)
            def _(c):
                these = span(c * fine, fine, fine)
                terms[i, 2, these, :] = (
                    terms[i, 2, these, :].astype(f32) + cross_in[i % 4, 1, these, :].astype(f32)
                ).astype(bf16)

            line_copy(i).start()
            cross_copy(i, 0).wait_recv()

    def line_step(i):
        g, b, same = pieces[i]
        q, yy = columns(i)

        @pl.when(owner(i))
        def _():
            line_copy(i).wait_recv()
            at = slab_at(q, yy)
            out_at = slab_at(b, yy)

            @pl.loop(0, rows // fine)
            def _(c):
                these = span(c * fine, fine, fine)
                total = terms[i, 0, these, :].astype(f32) + cross_in[i % 4, 0, these, :].astype(f32)
                total = total + line_in[i % 4, these, :].astype(f32)
                out_ref[these, out_at] = (middle[these, at].astype(f32) + total).astype(bf16)

    last = len(pieces) - 1
    for i in range(len(pieces)):
        if i == 2:
            across(1, 1).wait_recv()
            beside(1, 1, 1).start()
        term_step(i)
        if i >= 1:
            cross_step(i - 1)
        if i >= 2:
            line_step(i - 2)
    cross_step(last)
    line_step(last - 1)
    line_step(last)

    for copy in half_copies + sum_copies + part_copies + share_copies + middle_copies:
        copy.wait_send()
    for a in range(2):
        for k in range(3):
            swap(a, k).wait_send()
        for b in range(2):
            across(a, b).wait_send()
            for g in range(2):
                beside(a, g, b).wait_send()
    for q in range(LINES):
        for copy in gate_cross(q, y):
            copy.wait_send()
    for side, step in ((0, 1), (1, -1)):
        for d in range(LINES):
            q = z - step * d

            @pl.when((q >= 0) & (q < LINES) & (z + step >= 0) & (z + step < LINES))
            def _(q=q, side=side, step=step):
                for copy in gate_line(q, side, step):
                    copy.wait_send()

    for k in range(3):
        for i in range(steps):
            row_copy(k, i).wait_send()
            forward(k, i).wait_send()
    for n in range(4):
        for k in range(2):
            cross_copy(n, k).wait_send()
        line_copy(n).wait_send()
        term_copy(n).wait_send()


def fused_shards(fs, tokens, mixer_gain, w_content, w_spatial, content_scale, spatial_scale, spatial_gain,
                 block_mixing, block_bias, w_project, project_scale, channel_gain, w_up, up_scale, w_down, down_scale):
    rows, half = tokens.shape
    width = 2 * half
    channels = w_content.shape[1]
    share_width = channels // 2
    hidden_units = w_up.shape[1]
    units = hidden_units // 4
    depth = w_up.shape[0]
    slab = 2 * depth
    steps = rows // block_mixing.shape[1]
    bf16, f32 = jnp.bfloat16, jnp.float32
    sizes = dict(fine=64, tile=256, up_tile=256)
    vmem = pltpu.VMEM
    dma = pltpu.SemaphoreType.DMA
    row = lambda a: a.reshape(1, -1)
    sems = [(3,), (2,), None, None, (2, 3), (2, 2), (2, 2, 2), (3,), (2,), (steps,), (steps,), (3, steps), (3, steps),
            (4,), (4, 2), (4,)]
    pairs = []
    for shape in sems:
        if shape is not None:
            pairs += [dma(shape), dma(shape)]
        elif len(pairs) == 4:
            pairs += [dma((2, 2, LINES)), dma((2, LINES))]
        else:
            pairs += [dma((2, LINES)), dma((2, LINES))]
    return pl.pallas_call(
        functools.partial(layer_kernel, sizes),
        out_shape=jax.ShapeDtypeStruct((rows, half), bf16),
        in_specs=[
            pl.BlockSpec(memory_space=pl.ANY if i in (12, 14) else vmem) for i in range(16)
        ],
        out_specs=pl.BlockSpec(memory_space=vmem),
        scratch_shapes=[
            vmem((depth, hidden_units), f32),
            vmem((hidden_units, depth), f32),
            dma((2,)),
            vmem((2, rows, width), bf16),
            vmem((2, rows, width), bf16),
            vmem((width, 2 * share_width), bf16),
            vmem((share_width, width), bf16),
            vmem((depth, 2 * share_width), bf16),
            vmem((share_width, depth), bf16),
            vmem((depth, hidden_units), bf16),
            vmem((hidden_units, depth), bf16),
            vmem((width, units), bf16),
            vmem((units, width), bf16),
            vmem((2, rows, share_width), f32),
            vmem((2, rows, share_width), f32),
            vmem((2, rows, share_width), bf16),
            vmem((8, 128), f32),
            vmem((3, 8, 128), f32),
            vmem((2, rows, width), bf16),
            vmem((2, rows, half), bf16),
            vmem((rows, half), bf16),
            vmem((rows, half), bf16),
            vmem((rows, width), bf16),
            vmem((4, rows, width), bf16),
            vmem((4, rows, units), bf16),
            vmem((8, 4, rows, slab), bf16),
            vmem((4, 4, rows, slab), bf16),
            vmem((4, 2, rows, slab), bf16),
            vmem((4, rows, slab), bf16),
        ] + pairs,
        compiler_params=pltpu.CompilerParams(
            collective_id=0, has_side_effects=True, vmem_limit_bytes=VMEM_LIMIT
        ),
    )(tokens, row(mixer_gain), w_content, w_spatial, row(content_scale), row(spatial_scale), row(spatial_gain),
      block_mixing, block_bias, w_project, row(project_scale), row(channel_gain), w_up, row(up_scale), w_down,
      row(down_scale))


VMEM_LIMIT = 67043328


def solution(mesh):
    fs, tp = mesh.shape["fs"], mesh.shape["tp"]
    if tp == 2 and fs == LINES * PLANE:
        body = functools.partial(fused_shards, fs)
    else:
        body = shards
    return jax.shard_map(
        body,
        mesh=mesh,
        in_specs=(
            P("fs", "tp"),
            P(),
            P("fs", "tp"),
            P("fs", "tp"),
            P("tp"),
            P("tp"),
            P("tp"),
            P("tp", None, None),
            P("tp", None),
            P("tp", "fs"),
            P("fs"),
            P(),
            P("fs", "tp"),
            P("tp"),
            P("tp", "fs"),
            P("fs"),
        ),
        out_specs=P("fs", "tp"),
        check_vma=False,
    )
```

```python
import functools

import jax
import jax.numpy as jnp
from jax import lax
from jax.experimental import pallas as pl
from jax.experimental.pallas import tpu as pltpu
from jax.sharding import PartitionSpec as P

EPSILON = 1e-06


def normalize_rows(token_rows, gain_vector):
    values = token_rows.astype(jnp.float32)
    scaled = values * lax.rsqrt(jnp.mean(values * values, axis=-1, keepdims=True) + EPSILON)
    return (scaled * gain_vector).astype(jnp.bfloat16)


def shards(
    tokens,
    mixer_gain,
    w_content,
    w_spatial,
    content_scale,
    spatial_scale,
    spatial_gain,
    block_mixing,
    block_bias,
    w_project,
    project_scale,
    channel_gain,
    w_up,
    up_scale,
    w_down,
    down_scale,
):
    content_weight = w_content.astype(jnp.bfloat16)
    spatial_weight = w_spatial.astype(jnp.bfloat16)
    project_weight = w_project.astype(jnp.bfloat16)
    up_weight = w_up.astype(jnp.bfloat16)
    down_weight = w_down.astype(jnp.bfloat16)
    project_full, down_full = (
        lax.all_gather(project_scale, "fs", axis=0, tiled=True),
        lax.all_gather(down_scale, "fs", axis=0, tiled=True),
    )
    gathered_rows = lax.all_gather(tokens, "tp", axis=1, tiled=True)
    normed = normalize_rows(gathered_rows, mixer_gain)
    row_count = gathered_rows.shape[0]
    content_full, spatial_full, project_cols = (
        lax.all_gather(content_weight, "fs", axis=0, tiled=True),
        lax.all_gather(spatial_weight, "fs", axis=0, tiled=True),
        lax.all_gather(project_weight, "fs", axis=1, tiled=True),
    )
    content_linear = jnp.dot(normed, content_full, preferred_element_type=jnp.float32)
    spatial_linear = jnp.dot(normed, spatial_full, preferred_element_type=jnp.float32)
    content = jax.nn.gelu(content_linear * content_scale)
    spatial = jax.nn.gelu(spatial_linear * spatial_scale)
    square_sums = lax.psum(jnp.sum(spatial * spatial, axis=1), "tp")
    total_width = spatial.shape[1] * lax.axis_size("tp")
    spatial_norm = (
        spatial * lax.rsqrt(square_sums / total_width + EPSILON)[:, None] * spatial_gain
    ).astype(jnp.bfloat16)
    groups_here = block_mixing.shape[0]
    block_size = block_mixing.shape[1]
    group_width = spatial_norm.shape[1] // groups_here
    causal_mask = jnp.tril(jnp.ones((block_size, block_size), dtype=bool))
    mixing_weights = jnp.where(causal_mask[None, :, :], block_mixing, jnp.zeros_like(block_mixing))
    grouped = spatial_norm.reshape(row_count // block_size, block_size, groups_here, group_width)
    mixed_block = (
        jnp.einsum("gts,nsgc->ntgc", mixing_weights, grouped, preferred_element_type=jnp.float32)
        + block_bias.T[None, :, :, None]
    )
    gated = (content * mixed_block.reshape(row_count, spatial_norm.shape[1])).astype(jnp.bfloat16)
    mixer_terms = jnp.dot(gated, project_cols, preferred_element_type=jnp.float32) * project_full
    mixer_sum = lax.psum_scatter(
        mixer_terms.astype(jnp.bfloat16), "tp", scatter_dimension=1, tiled=True
    ).astype(jnp.float32)
    middle = (tokens.astype(jnp.float32) + mixer_sum).astype(jnp.bfloat16)
    middle_rows = lax.all_gather(middle, "tp", axis=1, tiled=True)
    channel_normed = normalize_rows(middle_rows, channel_gain)
    up_full, down_cols = (
        lax.all_gather(up_weight, "fs", axis=0, tiled=True),
        lax.all_gather(down_weight, "fs", axis=1, tiled=True),
    )
    up_linear = jnp.dot(channel_normed, up_full, preferred_element_type=jnp.float32)
    hidden = jnp.square(jax.nn.relu(up_linear * up_scale)).astype(jnp.bfloat16)
    channel_terms = jnp.dot(hidden, down_cols, preferred_element_type=jnp.float32) * down_full
    channel_sum = lax.psum_scatter(
        channel_terms.astype(jnp.bfloat16), "tp", scatter_dimension=1, tiled=True
    ).astype(jnp.float32)
    return (middle.astype(jnp.float32) + channel_sum).astype(jnp.bfloat16)


LINES = 4
PLANE = 4
MESH = pl.DeviceIdType.MESH


def layer_kernel(
    sizes,
    tokens_ref,
    mixer_gain_ref,
    content_ref,
    spatial_ref,
    content_scale_ref,
    spatial_scale_ref,
    spatial_gain_ref,
    mixing_ref,
    bias_ref,
    project_ref,
    project_scale_ref,
    channel_gain_ref,
    up_hbm,
    up_scale_ref,
    down_hbm,
    down_scale_ref,
    out_ref,
    up_ref,
    down_ref,
    load_sem,
    token_rows,
    normed,
    gate_weights,
    project_full,
    gate_other,
    project_other,
    up_own,
    down_own,
    up_full,
    down_full,
    content_buf,
    spatial_buf,
    gated,
    sums,
    sums_in,
    part,
    part_in,
    share,
    share_in,
    middle,
    rows_all,
    hidden,
    terms,
    terms_in,
    cross_in,
    line_in,
    token_send,
    token_recv,
    half_send,
    half_recv,
    gate_line_send,
    gate_line_recv,
    gate_send,
    gate_recv,
    swap_send,
    swap_recv,
    across_send,
    across_recv,
    beside_send,
    beside_recv,
    sum_send,
    sum_recv,
    part_send,
    part_recv,
    share_send,
    share_recv,
    middle_send,
    middle_recv,
    row_send,
    row_recv,
    fwd_send,
    fwd_recv,
    term_send,
    term_recv,
    cross_send,
    cross_recv,
    line_send,
    line_recv,
):
    rows, half = tokens_ref.shape
    width = 2 * half
    depth = content_ref.shape[0]
    channels = content_ref.shape[1]
    share_width = channels // 2
    units = up_full.shape[1]
    slab = 2 * depth
    fine = sizes["fine"]
    tile = sizes["tile"]
    groups, block_size = mixing_ref.shape[0], mixing_ref.shape[1]
    blocks = rows // block_size
    steps = rows // block_size
    me = lax.axis_index("fs")
    core = lax.axis_index("tp")
    z = me // PLANE
    p = me % PLANE
    y = p // 2
    x = p % 2
    zh = z // 2
    zl = z % 2
    other = 1 - core
    f32, bf16 = jnp.float32, jnp.bfloat16

    def span(start, size, by=128):
        return pl.ds(pl.multiple_of(start, by), size)

    beside_x = me + 1 - 2 * x
    beside_y = me + 2 - 4 * y
    beside_z = me + PLANE * (1 - 2 * zl)
    corner = beside_z + 1 - 2 * x
    far_z = me + 2 * PLANE * (1 - 2 * zh)
    inner = (z > 0) & (z < LINES - 1)
    pair = {"tp": other}
    mine = span(core * half, half)

    def remote(src, dst, send, recv, where):
        return pltpu.make_async_remote_copy(
            src_ref=src, dst_ref=dst, send_sem=send, recv_sem=recv, device_id=where, device_id_type=MESH
        )

    loads = [
        pltpu.make_async_copy(up_hbm, up_ref, load_sem.at[0]),
        pltpu.make_async_copy(down_hbm, down_ref, load_sem.at[1]),
    ]
    for load in loads:
        load.start()
    barrier = pltpu.get_barrier_semaphore()
    friends = [{"fs": i} for i in (beside_x, beside_y, beside_z, corner, far_z)]
    friends += [pair, {"fs": beside_x, "tp": other}]
    for friend in friends:
        pl.semaphore_signal(barrier, inc=1, device_id=friend, device_id_type=MESH)

    @pl.when(inner)
    def _():
        pl.semaphore_signal(
            barrier, inc=1, device_id={"fs": me + PLANE * (2 * zl - 1)}, device_id_type=MESH
        )

    own_channels = span(x * share_width, share_width)
    own_depth = span(me * depth, depth)

    def halves(channel_half, weights, project):
        at = span(channel_half * share_width, share_width)
        weights[:, pl.ds(0, share_width)] = content_ref[:, at].astype(bf16)
        weights[:, pl.ds(share_width, share_width)] = spatial_ref[:, at].astype(bf16)
        project[...] = (project_ref[at, :] * project_scale_ref[...]).astype(bf16)

    halves(1 - x, gate_other, project_other)
    halves(x, gate_weights.at[own_depth, :], project_full.at[:, own_depth])
    token_rows[0, :, mine] = tokens_ref[...]
    pl.semaphore_wait(barrier, len(friends) + inner.astype(jnp.int32))

    def slab_at(q, yy):
        return span((q * PLANE + yy * 2) * depth, slab)

    def gate_refs(q, yy, away):
        at = span((q * PLANE + yy * 2 + (1 - x if away else x)) * depth, depth)
        return gate_weights.at[at, :], project_full.at[:, at]

    def gate_line(q, side, step, away):
        refs = gate_refs(q, y, away)
        return [
            remote(
                refs[a], refs[a], gate_line_send.at[a, away, side, q], gate_line_recv.at[a, away, q],
                {"fs": me + step * PLANE},
            )
            for a in range(2)
        ]

    def gate_cross(q, yy, away):
        refs = gate_refs(q, yy, away)
        return [
            remote(refs[a], refs[a], gate_send.at[a, away, q], gate_recv.at[a, away, q], {"fs": beside_y})
            for a in range(2)
        ]

    def start_gate(away):
        for side, step in ((0, 1), (1, -1)):

            @pl.when((z + step >= 0) & (z + step < LINES))
            def _(side=side, step=step):
                for copy in gate_line(z, side, step, away):
                    copy.start()

        for copy in gate_cross(z, y, away):
            copy.start()

    half_copies = [
        remote(gate_other, gate_weights.at[own_depth, :], half_send.at[0], half_recv.at[0], {"fs": beside_x}),
        remote(project_other, project_full.at[:, own_depth], half_send.at[1], half_recv.at[1], {"fs": beside_x}),
    ]

    swap_to = (beside_x, beside_z, corner)
    swap_part = (2 * zl + 1 - x, 2 * (1 - zl) + x, 2 * (1 - zl) + 1 - x)

    def swap(a, k):
        theirs = span(swap_part[k] * units, units)
        src = up_own.at[:, theirs] if a == 0 else down_own.at[theirs, :]
        dst = up_full.at[own_depth, :] if a == 0 else down_full.at[:, own_depth]
        return remote(src, dst, swap_send.at[a, k], swap_recv.at[a, k], {"fs": swap_to[k]})

    def ff_ref(a, q, yy):
        return up_full.at[slab_at(q, yy), :] if a == 0 else down_full.at[:, slab_at(q, yy)]

    def line_of(g, b):
        return 2 * (zh if g == 0 else 1 - zh) + b

    def across(a, b):
        ref = ff_ref(a, line_of(0, b), y)
        return remote(ref, ref, across_send.at[a, b], across_recv.at[a, b], {"fs": far_z})

    def beside(a, g, b):
        ref = ff_ref(a, line_of(g, b), y)
        return remote(ref, ref, beside_send.at[a, g, b], beside_recv.at[a, g, b], {"fs": beside_y})

    def relay_gate(d, away):
        for side, step in ((0, 1), (1, -1)):
            q = z - step * d

            @pl.when((q >= 0) & (q < LINES))
            def _(q=q, side=side, step=step):
                for copy in gate_line(q, side, step, away):
                    copy.wait_recv()

                @pl.when((z + step >= 0) & (z + step < LINES))
                def _():
                    for copy in gate_line(q, side, step, away):
                        copy.start()

                for copy in gate_cross(q, y, away):
                    copy.start()

    for copy in half_copies:
        copy.start()
    start_gate(0)
    token_pair = remote(tokens_ref, token_rows.at[0, :, mine], token_send.at[0], token_recv.at[0], pair)
    token_pair.start()
    for load in loads:
        load.wait()

    @pl.loop(0, up_own.shape[1] // units)
    def _(j):
        up_own[:, span(j * units, units)] = up_ref[:, span(j * units, units)].astype(bf16)

    quarter = span((2 * zl + x) * units, units)
    swap(0, 0).start()
    token_cross = remote(
        tokens_ref, token_rows.at[1, :, mine], token_send.at[1], token_recv.at[1], {"fs": beside_x}
    )
    token_cross.start()
    up_full[own_depth, :] = up_ref[:, quarter].astype(bf16)

    @pl.loop(0, up_own.shape[1] // units)
    def _(j):
        down_own[span(j * units, units), :] = (
            down_ref[span(j * units, units), :] * down_scale_ref[...]
        ).astype(bf16)

    down_full[:, own_depth] = (down_ref[quarter, :] * down_scale_ref[...]).astype(bf16)

    for copy in half_copies:
        copy.wait_recv()
    start_gate(1)

    @pl.when(jnp.logical_not(inner))
    def _():
        swap(0, 1).start()
        swap(0, 2).start()

    def normalize(source, gain_ref, target, first, count):
        @pl.loop(0, count // fine)
        def _(i):
            these = span(first + i * fine, fine, fine)
            values = source[these, :].astype(f32)
            scaled = values * lax.rsqrt(jnp.mean(values * values, axis=-1, keepdims=True) + EPSILON)
            target[these, :] = (scaled * gain_ref[...]).astype(bf16)

    token_pair.wait()
    normalize(token_rows.at[0], mixer_gain_ref, normed.at[0], 0, rows)
    relay_gate(1, 0)
    relay_gate(1, 1)
    swap(0, 0).wait_recv()
    relay_gate(2, 0)
    relay_gate(2, 1)

    @pl.when(inner)
    def _():
        swap(0, 1).start()
        swap(0, 2).start()

    @pl.when(jnp.logical_not(inner))
    def _():
        across(0, zl).start()

    swap(1, 0).start()
    relay_gate(3, 0)
    relay_gate(3, 1)
    beside(0, 0, zl).start()
    token_cross.wait()

    @pl.when(inner)
    def _():
        across(0, zl).start()


    token_forward = remote(
        token_rows.at[1, :, mine], token_rows.at[1, :, mine], token_send.at[2], token_recv.at[2], pair
    )
    token_forward.start()
    token_forward.wait()
    normalize(token_rows.at[1], mixer_gain_ref, normed.at[1], 0, rows)

    def finish_up_swap():
        swap(0, 1).wait_recv()
        swap(0, 2).wait_recv()
        across(0, 1 - zl).start()
        beside(0, 0, 1 - zl).start()

    @pl.when(inner)
    def _():
        finish_up_swap()

    swap(1, 1).start()
    swap(1, 2).start()
    swap(1, 0).wait_recv()

    @pl.when(jnp.logical_not(inner))
    def _():
        across(1, zl).start()

    beside(1, 0, zl).start()

    def finish_down_swap():
        swap(1, 1).wait_recv()
        swap(1, 2).wait_recv()
        across(1, 1 - zl).start()

    for q in range(LINES):
        for away in range(2):
            for copy in gate_cross(q, 1 - y, away):
                copy.wait_recv()

    @pl.loop(0, 2)
    def _(s):
        linear = jnp.dot(normed[s], gate_weights[:, pl.ds(share_width, share_width)], preferred_element_type=f32)
        spatial_buf[s] = jax.nn.gelu(linear * spatial_scale_ref[:, own_channels])

    sums[...] = jnp.zeros_like(sums)
    for s in range(2):
        for n in range(blocks):
            values = spatial_buf[s, pl.ds(n * block_size, block_size), :]
            total = jnp.sum(values * values, axis=1, keepdims=True)
            sums[pl.ds(s * blocks + n, 1), :] = jnp.broadcast_to(total, (block_size, block_size)).T[:1, :]
    sum_to = (pair, {"fs": beside_x}, {"fs": beside_x, "tp": other})
    sum_copies = [remote(sums, sums_in.at[k], sum_send.at[k], sum_recv.at[k], sum_to[k]) for k in range(3)]
    for copy in sum_copies:
        copy.start()

    @pl.loop(0, 2)
    def _(s):
        linear = jnp.dot(normed[s], gate_weights[:, pl.ds(0, share_width)], preferred_element_type=f32)
        content_buf[s] = jax.nn.gelu(linear * content_scale_ref[:, own_channels])

    for copy in sum_copies:
        copy.wait_recv()

    causal = lax.broadcasted_iota(jnp.int32, (block_size, block_size), 0) >= lax.broadcasted_iota(
        jnp.int32, (block_size, block_size), 1
    )
    own_groups = groups // 2
    group_width = channels // groups
    part_copies = [
        remote(
            part.at[s, :, span(other * half, half)], part_in.at[s], part_send.at[s], part_recv.at[s], pair
        )
        for s in range(2)
    ]
    for s in (1, 0):
        for n in range(blocks):
            these = pl.ds(n * block_size, block_size)
            here, there = pl.ds(s * blocks + n, 1), pl.ds((1 - s) * blocks + n, 1)
            total = (sums[here, :] + sums_in[0, here, :]) + (sums_in[1, there, :] + sums_in[2, there, :])
            scale = lax.rsqrt(total / (2 * channels) + EPSILON)
            scale = jnp.broadcast_to(scale, (block_size, block_size)).T[:, :1]
            for g in range(own_groups):
                group = x * own_groups + g
                weights = jnp.where(causal, mixing_ref[group].astype(f32), 0.0).astype(bf16)
                bias = jnp.broadcast_to(bias_ref[pl.ds(group, 1), :], (block_size, block_size)).T[:, :1]
                at = pl.ds(g * group_width, group_width)
                gain = spatial_gain_ref[:, span(group * group_width, group_width)]
                spatial_norm = (spatial_buf[s, these, at] * scale * gain).astype(bf16)
                mixed = jnp.dot(weights, spatial_norm, preferred_element_type=f32) + bias
                gated[s, these, at] = (content_buf[s, these, at] * mixed).astype(bf16)

        @pl.loop(0, width // (2 * tile))
        def _(j, s=s):
            at = span(j * 2 * tile, 2 * tile)
            part[s, :, at] = jnp.dot(gated[s], project_full[:, at], preferred_element_type=f32).astype(bf16)

        part_copies[s].start()

    def step_rows(i):
        return pl.ds(i * block_size, block_size)

    share_copies = [
        remote(
            share.at[step_rows(i), :], share_in.at[step_rows(i), :], share_send.at[i], share_recv.at[i],
            {"fs": beside_x},
        )
        for i in range(steps)
    ]
    part_copies[1].wait_recv()
    for i in range(steps):
        these = step_rows(i)
        share[these, :] = (part[1, these, mine].astype(f32) + part_in[1, these, :].astype(f32)).astype(bf16)
        share_copies[i].start()
    part_copies[0].wait_recv()

    middle_copies = [
        remote(
            middle.at[step_rows(i), mine], middle.at[step_rows(i), mine], middle_send.at[i], middle_recv.at[i], pair
        )
        for i in range(steps)
    ]

    def row_copy(k, i):
        src = rows_all.at[2 if k == 2 else 0, step_rows(i), mine]
        dst = rows_all.at[k + 1, step_rows(i), mine]
        return remote(src, dst, row_send.at[k, i], row_recv.at[k, i], {"fs": beside_z if k == 1 else beside_x})

    def forward(k, i):
        ref = rows_all.at[k + 1, step_rows(i), mine]
        return remote(ref, ref, fwd_send.at[k, i], fwd_recv.at[k, i], pair)

    @pl.when(jnp.logical_not(inner))
    def _():
        finish_up_swap()

    for i in range(steps):
        these = step_rows(i)
        share_copies[i].wait_recv()
        total = part[0, these, mine].astype(f32) + part_in[0, these, :].astype(f32)
        total = total + share_in[these, :].astype(f32)
        middle[these, mine] = (tokens_ref[these, :].astype(f32) + total).astype(bf16)
        middle_copies[i].start()
        middle_copies[i].wait_recv()
        normalize(middle, channel_gain_ref, rows_all.at[0], i * block_size, block_size)
        row_copy(1, i).start()
        row_copy(0, i).start()
        if i == steps - 2:
            across(0, zl).wait_recv()
            beside(0, 1, zl).start()

    def pass_on(a, b):
        across(a, b).wait_recv()
        beside(a, 1, b).start()

    @pl.when(jnp.logical_not(inner))
    def _():
        pass_on(0, 1 - zl)

    for i in range(steps):
        row_copy(1, i).wait_recv()
        row_copy(2, i).start()
        forward(1, i).start()
        if i == 0:

            @pl.when(jnp.logical_not(inner))
            def _():
                finish_down_swap()

            @pl.when(inner)
            def _():
                pass_on(0, 1 - zl)

        if i == steps - 2:

            @pl.when(inner)
            def _():
                across(1, zl).start()

    @pl.when(inner)
    def _():
        finish_down_swap()

    beside(1, 0, 1 - zl).start()

    @pl.when(inner)
    def _():
        pass_on(1, zl)

    for i in range(steps):
        row_copy(0, i).wait_recv()
        forward(0, i).start()
    for g in range(2):
        for b in range(2):
            beside(0, g, b).wait_recv()

    up_tile = sizes["up_tile"]
    unit_base = (2 * zl + x) * units

    def up_product(r):
        @pl.loop(0, units // up_tile)
        def _(j):
            at = span(j * up_tile, up_tile)
            linear = jnp.dot(rows_all[r], up_full[:, at], preferred_element_type=f32)
            linear = linear * up_scale_ref[:, span(unit_base + j * up_tile, up_tile)]
            hidden[r, :, at] = jnp.square(jnp.maximum(linear, 0.0)).astype(bf16)

    up_product(0)
    for k in range(2):
        for i in range(steps):
            forward(k, i).wait_recv()
        up_product(k + 1)

    @pl.when(jnp.logical_not(inner))
    def _():
        pass_on(1, zl)

    @pl.when(inner)
    def _():
        pass_on(1, 1 - zl)


    pieces = [(g, same, late) for g in range(2) for same in range(2) for late in range(2)]

    def bit(i):
        g, same, late = pieces[i]
        if g == 0 or same == 0:
            return late
        return zl if late == 0 else 1 - zl

    def place(i):
        g, same, _ = pieces[i]
        n = 2 * same + bit(i)
        return 4 * g + n, n

    def columns(i):
        g, same, _ = pieces[i]
        return line_of(g, bit(i)), y if same == 0 else 1 - y

    def owner(i):
        return (zh if pieces[i][0] == 0 else 1 - zh) == core

    def term_copy(i, k):
        at, n = place(i)
        src, dst = (terms.at[at, 3], terms_in.at[n, 3]) if k else (terms.at[at, 0:3], terms_in.at[n, 0:3])
        return remote(src, dst, term_send.at[n, k], term_recv.at[n, k], pair)

    def routes(i):
        return (1, beside_x, 2, beside_z) if pieces[i][0] == 0 else (2, beside_z, 1, beside_x)

    def cross_copy(i, k):
        at, n = place(i)
        slot, to, _, _ = routes(i)
        src = terms.at[at, 3 if k else slot]
        return remote(src, cross_in.at[n, k], cross_send.at[n, k], cross_recv.at[n, k], {"fs": to})

    def line_copy(i):
        at, n = place(i)
        _, _, slot, to = routes(i)
        return remote(terms.at[at, slot], line_in.at[n], line_send.at[n], line_recv.at[n], {"fs": to})

    def product_step(i, k):
        g, same, _ = pieces[i]
        if same == 1 and k == 0:
            beside(1, g, bit(i)).wait_recv()
        at, _ = place(i)
        q, yy = columns(i)

        def product(r):
            terms[at, r] = jnp.dot(hidden[r], down_full[:, slab_at(q, yy)], preferred_element_type=f32).astype(bf16)

        if k == 0:
            pl.loop(0, 3)(product)
        else:
            product(3)

        @pl.when(jnp.logical_not(owner(i)))
        def _():
            term_copy(i, k).start()

    def add_step(i, k):
        at, n = place(i)

        @pl.when(owner(i))
        def _():
            term_copy(i, k).wait_recv()

            def add(r):
                @pl.loop(0, rows // fine)
                def _(c):
                    these = span(c * fine, fine, fine)
                    terms[at, r, these, :] = (
                        terms[at, r, these, :].astype(f32) + terms_in[n, r, these, :].astype(f32)
                    ).astype(bf16)

            first, _, second, _ = routes(i)
            if k == 1:
                add(3)
                cross_copy(i, 1).start()
            else:
                add(first)
                cross_copy(i, 0).start()
                add(second)
                add(0)

    def cross_step(i):
        at, n = place(i)

        @pl.when(owner(i))
        def _():
            cross_copy(i, 1).wait_recv()
            slot = routes(i)[2]

            @pl.loop(0, rows // fine)
            def _(c):
                these = span(c * fine, fine, fine)
                terms[at, slot, these, :] = (
                    terms[at, slot, these, :].astype(f32) + cross_in[n, 1, these, :].astype(f32)
                ).astype(bf16)

            line_copy(i).start()
            cross_copy(i, 0).wait_recv()

    def line_step(i):
        at, n = place(i)
        q, yy = columns(i)

        @pl.when(owner(i))
        def _():
            line_copy(i).wait_recv()
            out_at = slab_at(q % 2, yy)

            @pl.loop(0, rows // fine)
            def _(c):
                these = span(c * fine, fine, fine)
                total = terms[at, 0, these, :].astype(f32) + cross_in[n, 0, these, :].astype(f32)
                total = total + line_in[n, these, :].astype(f32)
                out_ref[these, out_at] = (middle[these, slab_at(q, yy)].astype(f32) + total).astype(bf16)

    def far_step(i):
        @pl.when(jnp.logical_not(inner))
        def _():
            pass_on(1, 1 - zl)

    def run_tail(names):
        kinds = dict(
            p=lambda i: (product_step(i, 0), product_step(i, 1)),
            q=lambda i: product_step(i, 0),
            r=lambda i: product_step(i, 1),
            a=lambda i: (add_step(i, 0), add_step(i, 1)),
            b=lambda i: add_step(i, 0),
            d=lambda i: add_step(i, 1),
            c=cross_step,
            l=line_step,
            f=far_step,
        )
        for name in names:
            kinds[name[0]](int(name[1]))

    run_tail(sizes["early"])
    for i in range(steps):
        row_copy(2, i).wait_recv()
        forward(2, i).start()
    for i in range(steps):
        forward(2, i).wait_recv()
    up_product(3)
    run_tail(sizes["late"])

    for copy in half_copies + sum_copies + part_copies + share_copies + middle_copies:
        copy.wait_send()
    for a in range(2):
        for k in range(3):
            swap(a, k).wait_send()
        for b in range(2):
            across(a, b).wait_send()
            for g in range(2):
                beside(a, g, b).wait_send()
    for q in range(LINES):
        for away in range(2):
            for copy in gate_cross(q, y, away):
                copy.wait_send()
    for side, step in ((0, 1), (1, -1)):
        for d in range(LINES):
            q = z - step * d

            @pl.when((q >= 0) & (q < LINES) & (z + step >= 0) & (z + step < LINES))
            def _(q=q, side=side, step=step):
                for away in range(2):
                    for copy in gate_line(q, side, step, away):
                        copy.wait_send()

    for k in range(3):
        for i in range(steps):
            row_copy(k, i).wait_send()
            forward(k, i).wait_send()
    for i in range(4):
        for k in range(2):
            cross_copy(i, k).wait_send()
        line_copy(i).wait_send()
        for k in range(2):
            term_copy(i, k).wait_send()


def fused_shards(fs, tokens, mixer_gain, w_content, w_spatial, content_scale, spatial_scale, spatial_gain,
                 block_mixing, block_bias, w_project, project_scale, channel_gain, w_up, up_scale, w_down, down_scale):
    rows, half = tokens.shape
    width = 2 * half
    channels = w_content.shape[1]
    share_width = channels // 2
    hidden_units = w_up.shape[1]
    units = hidden_units // 4
    depth = w_up.shape[0]
    slab = 2 * depth
    steps = rows // block_mixing.shape[1]
    bf16, f32 = jnp.bfloat16, jnp.float32
    early = [
        "q0", "q2",
    ]
    late = [
        "r0", "b0", "r2", "d0", "f1", "p4", "b2", "d2", "p5", "a4", "p1", "a5", "p3", "a1", "p6", "a3", "c0",
        "a6", "c4", "c2", "p7", "a7", "c5", "c1", "c6", "c3", "c7", "l0", "l2", "l4", "l5", "l1", "l3", "l6",
        "l7",
    ]
    sizes = dict(fine=64, tile=256, up_tile=256, early=early, late=late)
    vmem = pltpu.VMEM
    dma = pltpu.SemaphoreType.DMA
    row = lambda a: a.reshape(1, -1)
    sems = [(3,), (2,), None, None, (2, 3), (2, 2), (2, 2, 2), (3,), (2,), (steps,), (steps,), (3, steps), (3, steps),
            (4, 2), (4, 2), (4,)]
    pairs = []
    for shape in sems:
        if shape is not None:
            pairs += [dma(shape), dma(shape)]
        elif len(pairs) == 4:
            pairs += [dma((2, 2, 2, LINES)), dma((2, 2, LINES))]
        else:
            pairs += [dma((2, 2, LINES)), dma((2, 2, LINES))]
    return pl.pallas_call(
        functools.partial(layer_kernel, sizes),
        out_shape=jax.ShapeDtypeStruct((rows, half), bf16),
        in_specs=[
            pl.BlockSpec(memory_space=pl.ANY if i in (12, 14) else vmem) for i in range(16)
        ],
        out_specs=pl.BlockSpec(memory_space=vmem),
        scratch_shapes=[
            vmem((depth, hidden_units), f32),
            vmem((hidden_units, depth), f32),
            dma((2,)),
            vmem((2, rows, width), bf16),
            vmem((2, rows, width), bf16),
            vmem((width, 2 * share_width), bf16),
            vmem((share_width, width), bf16),
            vmem((depth, 2 * share_width), bf16),
            vmem((share_width, depth), bf16),
            vmem((depth, hidden_units), bf16),
            vmem((hidden_units, depth), bf16),
            vmem((width, units), bf16),
            vmem((units, width), bf16),
            vmem((2, rows, share_width), f32),
            vmem((2, rows, share_width), f32),
            vmem((2, rows, share_width), bf16),
            vmem((8, 128), f32),
            vmem((3, 8, 128), f32),
            vmem((2, rows, width), bf16),
            vmem((2, rows, half), bf16),
            vmem((rows, half), bf16),
            vmem((rows, half), bf16),
            vmem((rows, width), bf16),
            vmem((4, rows, width), bf16),
            vmem((4, rows, units), bf16),
            vmem((8, 4, rows, slab), bf16),
            vmem((4, 4, rows, slab), bf16),
            vmem((4, 2, rows, slab), bf16),
            vmem((4, rows, slab), bf16),
        ] + pairs,
        compiler_params=pltpu.CompilerParams(
            collective_id=0, has_side_effects=True, vmem_limit_bytes=VMEM_LIMIT
        ),
    )(tokens, row(mixer_gain), w_content, w_spatial, row(content_scale), row(spatial_scale), row(spatial_gain),
      block_mixing, block_bias, w_project, row(project_scale), row(channel_gain), w_up, row(up_scale), w_down,
      row(down_scale))


VMEM_LIMIT = 67043328


def solution(mesh):
    fs, tp = mesh.shape["fs"], mesh.shape["tp"]
    if tp == 2 and fs == LINES * PLANE:
        body = functools.partial(fused_shards, fs)
    else:
        body = shards
    return jax.shard_map(
        body,
        mesh=mesh,
        in_specs=(
            P("fs", "tp"),
            P(),
            P("fs", "tp"),
            P("fs", "tp"),
            P("tp"),
            P("tp"),
            P("tp"),
            P("tp", None, None),
            P("tp", None),
            P("tp", "fs"),
            P("fs"),
            P(),
            P("fs", "tp"),
            P("tp"),
            P("tp", "fs"),
            P("fs"),
        ),
        out_specs=P("fs", "tp"),
        check_vma=False,
    )
```

```python
import functools

import jax
import jax.numpy as jnp
from jax import lax
from jax.experimental import pallas as pl
from jax.experimental.pallas import tpu as pltpu
from jax.sharding import PartitionSpec as P

EPSILON = 1e-06


def normalize_rows(token_rows, gain_vector):
    values = token_rows.astype(jnp.float32)
    scaled = values * lax.rsqrt(jnp.mean(values * values, axis=-1, keepdims=True) + EPSILON)
    return (scaled * gain_vector).astype(jnp.bfloat16)


def shards(
    tokens,
    mixer_gain,
    w_content,
    w_spatial,
    content_scale,
    spatial_scale,
    spatial_gain,
    block_mixing,
    block_bias,
    w_project,
    project_scale,
    channel_gain,
    w_up,
    up_scale,
    w_down,
    down_scale,
):
    content_weight = w_content.astype(jnp.bfloat16)
    spatial_weight = w_spatial.astype(jnp.bfloat16)
    project_weight = w_project.astype(jnp.bfloat16)
    up_weight = w_up.astype(jnp.bfloat16)
    down_weight = w_down.astype(jnp.bfloat16)
    project_full, down_full = (
        lax.all_gather(project_scale, "fs", axis=0, tiled=True),
        lax.all_gather(down_scale, "fs", axis=0, tiled=True),
    )
    gathered_rows = lax.all_gather(tokens, "tp", axis=1, tiled=True)
    normed = normalize_rows(gathered_rows, mixer_gain)
    row_count = gathered_rows.shape[0]
    content_full, spatial_full, project_cols = (
        lax.all_gather(content_weight, "fs", axis=0, tiled=True),
        lax.all_gather(spatial_weight, "fs", axis=0, tiled=True),
        lax.all_gather(project_weight, "fs", axis=1, tiled=True),
    )
    content_linear = jnp.dot(normed, content_full, preferred_element_type=jnp.float32)
    spatial_linear = jnp.dot(normed, spatial_full, preferred_element_type=jnp.float32)
    content = jax.nn.gelu(content_linear * content_scale)
    spatial = jax.nn.gelu(spatial_linear * spatial_scale)
    square_sums = lax.psum(jnp.sum(spatial * spatial, axis=1), "tp")
    total_width = spatial.shape[1] * lax.axis_size("tp")
    spatial_norm = (
        spatial * lax.rsqrt(square_sums / total_width + EPSILON)[:, None] * spatial_gain
    ).astype(jnp.bfloat16)
    groups_here = block_mixing.shape[0]
    block_size = block_mixing.shape[1]
    group_width = spatial_norm.shape[1] // groups_here
    causal_mask = jnp.tril(jnp.ones((block_size, block_size), dtype=bool))
    mixing_weights = jnp.where(causal_mask[None, :, :], block_mixing, jnp.zeros_like(block_mixing))
    grouped = spatial_norm.reshape(row_count // block_size, block_size, groups_here, group_width)
    mixed_block = (
        jnp.einsum("gts,nsgc->ntgc", mixing_weights, grouped, preferred_element_type=jnp.float32)
        + block_bias.T[None, :, :, None]
    )
    gated = (content * mixed_block.reshape(row_count, spatial_norm.shape[1])).astype(jnp.bfloat16)
    mixer_terms = jnp.dot(gated, project_cols, preferred_element_type=jnp.float32) * project_full
    mixer_sum = lax.psum_scatter(
        mixer_terms.astype(jnp.bfloat16), "tp", scatter_dimension=1, tiled=True
    ).astype(jnp.float32)
    middle = (tokens.astype(jnp.float32) + mixer_sum).astype(jnp.bfloat16)
    middle_rows = lax.all_gather(middle, "tp", axis=1, tiled=True)
    channel_normed = normalize_rows(middle_rows, channel_gain)
    up_full, down_cols = (
        lax.all_gather(up_weight, "fs", axis=0, tiled=True),
        lax.all_gather(down_weight, "fs", axis=1, tiled=True),
    )
    up_linear = jnp.dot(channel_normed, up_full, preferred_element_type=jnp.float32)
    hidden = jnp.square(jax.nn.relu(up_linear * up_scale)).astype(jnp.bfloat16)
    channel_terms = jnp.dot(hidden, down_cols, preferred_element_type=jnp.float32) * down_full
    channel_sum = lax.psum_scatter(
        channel_terms.astype(jnp.bfloat16), "tp", scatter_dimension=1, tiled=True
    ).astype(jnp.float32)
    return (middle.astype(jnp.float32) + channel_sum).astype(jnp.bfloat16)


LINES = 4
PLANE = 4
MESH = pl.DeviceIdType.MESH


def layer_kernel(
    sizes,
    tokens_ref,
    mixer_gain_ref,
    content_ref,
    spatial_ref,
    content_scale_ref,
    spatial_scale_ref,
    spatial_gain_ref,
    mixing_ref,
    bias_ref,
    project_ref,
    project_scale_ref,
    channel_gain_ref,
    up_hbm,
    up_scale_ref,
    down_hbm,
    down_scale_ref,
    out_ref,
    up_ref,
    down_ref,
    load_sem,
    token_rows,
    normed,
    gate_weights,
    project_full,
    gate_other,
    project_other,
    up_own,
    down_own,
    up_full,
    down_full,
    content_buf,
    spatial_buf,
    gated,
    sums,
    sums_in,
    part,
    part_in,
    share,
    share_in,
    middle,
    rows_all,
    hidden,
    terms,
    terms_in,
    cross_in,
    line_in,
    token_send,
    token_recv,
    half_send,
    half_recv,
    gate_line_send,
    gate_line_recv,
    gate_send,
    gate_recv,
    swap_send,
    swap_recv,
    across_send,
    across_recv,
    beside_send,
    beside_recv,
    sum_send,
    sum_recv,
    part_send,
    part_recv,
    share_send,
    share_recv,
    middle_send,
    middle_recv,
    row_send,
    row_recv,
    fwd_send,
    fwd_recv,
    term_send,
    term_recv,
    cross_send,
    cross_recv,
    line_send,
    line_recv,
):
    rows, half = tokens_ref.shape
    width = 2 * half
    depth = content_ref.shape[0]
    channels = content_ref.shape[1]
    share_width = channels // 2
    units = up_full.shape[1]
    slab = 2 * depth
    fine = sizes["fine"]
    tile = sizes["tile"]
    groups, block_size = mixing_ref.shape[0], mixing_ref.shape[1]
    blocks = rows // block_size
    steps = rows // block_size
    me = lax.axis_index("fs")
    core = lax.axis_index("tp")
    z = me // PLANE
    p = me % PLANE
    y = p // 2
    x = p % 2
    zh = z // 2
    zl = z % 2
    other = 1 - core
    f32, bf16 = jnp.float32, jnp.bfloat16

    def span(start, size, by=128):
        return pl.ds(pl.multiple_of(start, by), size)

    beside_x = me + 1 - 2 * x
    beside_y = me + 2 - 4 * y
    beside_z = me + PLANE * (1 - 2 * zl)
    corner = beside_z + 1 - 2 * x
    far_z = me + 2 * PLANE * (1 - 2 * zh)
    inner = (z > 0) & (z < LINES - 1)
    pair = {"tp": other}
    mine = span(core * half, half)

    def remote(src, dst, send, recv, where):
        return pltpu.make_async_remote_copy(
            src_ref=src, dst_ref=dst, send_sem=send, recv_sem=recv, device_id=where, device_id_type=MESH
        )

    loads = [
        pltpu.make_async_copy(up_hbm, up_ref, load_sem.at[0]),
        pltpu.make_async_copy(down_hbm, down_ref, load_sem.at[1]),
    ]
    for load in loads:
        load.start()
    barrier = pltpu.get_barrier_semaphore()
    friends = [{"fs": i} for i in (beside_x, beside_y, beside_z, corner, far_z)]
    friends += [pair, {"fs": beside_x, "tp": other}]
    for friend in friends:
        pl.semaphore_signal(barrier, inc=1, device_id=friend, device_id_type=MESH)

    @pl.when(inner)
    def _():
        pl.semaphore_signal(
            barrier, inc=1, device_id={"fs": me + PLANE * (2 * zl - 1)}, device_id_type=MESH
        )

    own_channels = span(x * share_width, share_width)
    own_depth = span(me * depth, depth)

    def halves(channel_half, weights, project):
        at = span(channel_half * share_width, share_width)
        weights[:, pl.ds(0, share_width)] = content_ref[:, at].astype(bf16)
        weights[:, pl.ds(share_width, share_width)] = spatial_ref[:, at].astype(bf16)
        project[...] = (project_ref[at, :] * project_scale_ref[...]).astype(bf16)

    halves(1 - x, gate_other, project_other)
    halves(x, gate_weights.at[own_depth, :], project_full.at[:, own_depth])
    token_rows[0, :, mine] = tokens_ref[...]
    pl.semaphore_wait(barrier, len(friends) + inner.astype(jnp.int32))

    def slab_at(q, yy):
        return span((q * PLANE + yy * 2) * depth, slab)

    def gate_refs(q, yy, away):
        at = span((q * PLANE + yy * 2 + (1 - x if away else x)) * depth, depth)
        return gate_weights.at[at, :], project_full.at[:, at]

    def gate_line(q, side, step, away):
        refs = gate_refs(q, y, away)
        return [
            remote(
                refs[a], refs[a], gate_line_send.at[a, away, side, q], gate_line_recv.at[a, away, q],
                {"fs": me + step * PLANE},
            )
            for a in range(2)
        ]

    def gate_cross(q, yy, away):
        refs = gate_refs(q, yy, away)
        return [
            remote(refs[a], refs[a], gate_send.at[a, away, q], gate_recv.at[a, away, q], {"fs": beside_y})
            for a in range(2)
        ]

    def start_gate(away):
        for side, step in ((0, 1), (1, -1)):

            @pl.when((z + step >= 0) & (z + step < LINES))
            def _(side=side, step=step):
                for copy in gate_line(z, side, step, away):
                    copy.start()

        for copy in gate_cross(z, y, away):
            copy.start()

    half_copies = [
        remote(gate_other, gate_weights.at[own_depth, :], half_send.at[0], half_recv.at[0], {"fs": beside_x}),
        remote(project_other, project_full.at[:, own_depth], half_send.at[1], half_recv.at[1], {"fs": beside_x}),
    ]

    swap_to = (beside_x, beside_z, corner)
    swap_part = (2 * zl + 1 - x, 2 * (1 - zl) + x, 2 * (1 - zl) + 1 - x)

    def swap(a, k):
        theirs = span(swap_part[k] * units, units)
        src = up_own.at[:, theirs] if a == 0 else down_own.at[theirs, :]
        dst = up_full.at[own_depth, :] if a == 0 else down_full.at[:, own_depth]
        return remote(src, dst, swap_send.at[a, k], swap_recv.at[a, k], {"fs": swap_to[k]})

    def ff_ref(a, q, yy):
        return up_full.at[slab_at(q, yy), :] if a == 0 else down_full.at[:, slab_at(q, yy)]

    def line_of(g, b):
        return 2 * (zh if g == 0 else 1 - zh) + b

    def across(a, b):
        ref = ff_ref(a, line_of(0, b), y)
        return remote(ref, ref, across_send.at[a, b], across_recv.at[a, b], {"fs": far_z})

    def beside(a, g, b):
        ref = ff_ref(a, line_of(g, b), y)
        return remote(ref, ref, beside_send.at[a, g, b], beside_recv.at[a, g, b], {"fs": beside_y})

    def relay_gate(d, away):
        for side, step in ((0, 1), (1, -1)):
            q = z - step * d

            @pl.when((q >= 0) & (q < LINES))
            def _(q=q, side=side, step=step):
                for copy in gate_line(q, side, step, away):
                    copy.wait_recv()

                @pl.when((z + step >= 0) & (z + step < LINES))
                def _():
                    for copy in gate_line(q, side, step, away):
                        copy.start()

                for copy in gate_cross(q, y, away):
                    copy.start()

    for copy in half_copies:
        copy.start()
    start_gate(0)
    token_pair = remote(tokens_ref, token_rows.at[0, :, mine], token_send.at[0], token_recv.at[0], pair)
    token_pair.start()
    for load in loads:
        load.wait()

    @pl.loop(0, up_own.shape[1] // units)
    def _(j):
        up_own[:, span(j * units, units)] = up_ref[:, span(j * units, units)].astype(bf16)

    quarter = span((2 * zl + x) * units, units)
    swap(0, 0).start()
    token_cross = remote(
        tokens_ref, token_rows.at[1, :, mine], token_send.at[1], token_recv.at[1], {"fs": beside_x}
    )
    token_cross.start()
    up_full[own_depth, :] = up_ref[:, quarter].astype(bf16)

    @pl.loop(0, up_own.shape[1] // units)
    def _(j):
        down_own[span(j * units, units), :] = (
            down_ref[span(j * units, units), :] * down_scale_ref[...]
        ).astype(bf16)

    down_full[:, own_depth] = (down_ref[quarter, :] * down_scale_ref[...]).astype(bf16)

    for copy in half_copies:
        copy.wait_recv()
    start_gate(1)

    @pl.when(jnp.logical_not(inner))
    def _():
        swap(0, 1).start()
        swap(0, 2).start()

    def normalize(source, gain_ref, target, first, count):
        @pl.loop(0, count // fine)
        def _(i):
            these = span(first + i * fine, fine, fine)
            values = source[these, :].astype(f32)
            scaled = values * lax.rsqrt(jnp.mean(values * values, axis=-1, keepdims=True) + EPSILON)
            target[these, :] = (scaled * gain_ref[...]).astype(bf16)

    token_pair.wait()
    normalize(token_rows.at[0], mixer_gain_ref, normed.at[0], 0, rows)
    relay_gate(1, 0)
    relay_gate(1, 1)
    swap(0, 0).wait_recv()
    relay_gate(2, 0)
    relay_gate(2, 1)

    @pl.when(inner)
    def _():
        swap(0, 1).start()
        swap(0, 2).start()

    @pl.when(jnp.logical_not(inner))
    def _():
        across(0, zl).start()

    swap(1, 0).start()
    relay_gate(3, 0)
    relay_gate(3, 1)
    beside(0, 0, zl).start()
    token_cross.wait()

    @pl.when(inner)
    def _():
        across(0, zl).start()


    token_forward = remote(
        token_rows.at[1, :, mine], token_rows.at[1, :, mine], token_send.at[2], token_recv.at[2], pair
    )
    token_forward.start()
    token_forward.wait()
    normalize(token_rows.at[1], mixer_gain_ref, normed.at[1], 0, rows)

    def finish_up_swap():
        swap(0, 1).wait_recv()
        swap(0, 2).wait_recv()
        across(0, 1 - zl).start()
        beside(0, 0, 1 - zl).start()

    @pl.when(inner)
    def _():
        finish_up_swap()

    swap(1, 1).start()
    swap(1, 2).start()
    swap(1, 0).wait_recv()

    @pl.when(jnp.logical_not(inner))
    def _():
        across(1, zl).start()

    beside(1, 0, zl).start()

    def finish_down_swap():
        swap(1, 1).wait_recv()
        swap(1, 2).wait_recv()
        across(1, 1 - zl).start()

    for q in range(LINES):
        for away in range(2):
            for copy in gate_cross(q, 1 - y, away):
                copy.wait_recv()

    @pl.loop(0, 2)
    def _(s):
        linear = jnp.dot(normed[s], gate_weights[:, pl.ds(share_width, share_width)], preferred_element_type=f32)
        spatial_buf[s] = jax.nn.gelu(linear * spatial_scale_ref[:, own_channels])

    sums[...] = jnp.zeros_like(sums)
    for s in range(2):
        for n in range(blocks):
            values = spatial_buf[s, pl.ds(n * block_size, block_size), :]
            total = jnp.sum(values * values, axis=1, keepdims=True)
            sums[pl.ds(s * blocks + n, 1), :] = jnp.broadcast_to(total, (block_size, block_size)).T[:1, :]
    sum_to = (pair, {"fs": beside_x}, {"fs": beside_x, "tp": other})
    sum_copies = [remote(sums, sums_in.at[k], sum_send.at[k], sum_recv.at[k], sum_to[k]) for k in range(3)]
    for copy in sum_copies:
        copy.start()

    @pl.loop(0, 2)
    def _(s):
        linear = jnp.dot(normed[s], gate_weights[:, pl.ds(0, share_width)], preferred_element_type=f32)
        content_buf[s] = jax.nn.gelu(linear * content_scale_ref[:, own_channels])

    for copy in sum_copies:
        copy.wait_recv()

    causal = lax.broadcasted_iota(jnp.int32, (block_size, block_size), 0) >= lax.broadcasted_iota(
        jnp.int32, (block_size, block_size), 1
    )
    own_groups = groups // 2
    group_width = channels // groups
    part_copies = [
        remote(
            part.at[s, :, span(other * half, half)], part_in.at[s], part_send.at[s], part_recv.at[s], pair
        )
        for s in range(2)
    ]
    for s in (1, 0):
        for n in range(blocks):
            these = pl.ds(n * block_size, block_size)
            here, there = pl.ds(s * blocks + n, 1), pl.ds((1 - s) * blocks + n, 1)
            total = (sums[here, :] + sums_in[0, here, :]) + (sums_in[1, there, :] + sums_in[2, there, :])
            scale = lax.rsqrt(total / (2 * channels) + EPSILON)
            scale = jnp.broadcast_to(scale, (block_size, block_size)).T[:, :1]
            for g in range(own_groups):
                group = x * own_groups + g
                weights = jnp.where(causal, mixing_ref[group].astype(f32), 0.0).astype(bf16)
                bias = jnp.broadcast_to(bias_ref[pl.ds(group, 1), :], (block_size, block_size)).T[:, :1]
                at = pl.ds(g * group_width, group_width)
                gain = spatial_gain_ref[:, span(group * group_width, group_width)]
                spatial_norm = (spatial_buf[s, these, at] * scale * gain).astype(bf16)
                mixed = jnp.dot(weights, spatial_norm, preferred_element_type=f32) + bias
                gated[s, these, at] = (content_buf[s, these, at] * mixed).astype(bf16)

        @pl.loop(0, width // (2 * tile))
        def _(j, s=s):
            at = span(j * 2 * tile, 2 * tile)
            part[s, :, at] = jnp.dot(gated[s], project_full[:, at], preferred_element_type=f32).astype(bf16)

        part_copies[s].start()

    def step_rows(i):
        return pl.ds(i * block_size, block_size)

    share_copies = [
        remote(
            share.at[step_rows(i), :], share_in.at[step_rows(i), :], share_send.at[i], share_recv.at[i],
            {"fs": beside_x},
        )
        for i in range(steps)
    ]
    part_copies[1].wait_recv()
    for i in range(steps):
        these = step_rows(i)
        share[these, :] = (part[1, these, mine].astype(f32) + part_in[1, these, :].astype(f32)).astype(bf16)
        share_copies[i].start()
    part_copies[0].wait_recv()

    middle_copies = [
        remote(
            middle.at[step_rows(i), mine], middle.at[step_rows(i), mine], middle_send.at[i], middle_recv.at[i], pair
        )
        for i in range(steps)
    ]

    def row_copy(k, i):
        src = rows_all.at[2 if k == 2 else 0, step_rows(i), mine]
        dst = rows_all.at[k + 1, step_rows(i), mine]
        return remote(src, dst, row_send.at[k, i], row_recv.at[k, i], {"fs": beside_z if k == 1 else beside_x})

    def forward(k, i):
        ref = rows_all.at[k + 1, step_rows(i), mine]
        return remote(ref, ref, fwd_send.at[k, i], fwd_recv.at[k, i], pair)

    @pl.when(jnp.logical_not(inner))
    def _():
        finish_up_swap()

    for i in range(steps):
        these = step_rows(i)
        share_copies[i].wait_recv()
        total = part[0, these, mine].astype(f32) + part_in[0, these, :].astype(f32)
        total = total + share_in[these, :].astype(f32)
        middle[these, mine] = (tokens_ref[these, :].astype(f32) + total).astype(bf16)
        middle_copies[i].start()
        middle_copies[i].wait_recv()
        normalize(middle, channel_gain_ref, rows_all.at[0], i * block_size, block_size)
        row_copy(1, i).start()
        row_copy(0, i).start()
        if i == steps - 2:
            across(0, zl).wait_recv()
            beside(0, 1, zl).start()

    def pass_on(a, b):
        across(a, b).wait_recv()
        beside(a, 1, b).start()

    @pl.when(jnp.logical_not(inner))
    def _():
        pass_on(0, 1 - zl)

    for i in range(steps):
        row_copy(1, i).wait_recv()
        row_copy(2, i).start()
        forward(1, i).start()
        if i == 0:

            @pl.when(jnp.logical_not(inner))
            def _():
                finish_down_swap()

            @pl.when(inner)
            def _():
                pass_on(0, 1 - zl)

        if i == steps - 2:

            @pl.when(inner)
            def _():
                across(1, zl).start()

    @pl.when(inner)
    def _():
        finish_down_swap()

    beside(1, 0, 1 - zl).start()

    @pl.when(inner)
    def _():
        pass_on(1, zl)

    for i in range(steps):
        row_copy(0, i).wait_recv()
        forward(0, i).start()
    for g in range(2):
        for b in range(2):
            beside(0, g, b).wait_recv()

    up_tile = sizes["up_tile"]
    unit_base = (2 * zl + x) * units

    def up_product(r):
        @pl.loop(0, units // up_tile)
        def _(j):
            at = span(j * up_tile, up_tile)
            linear = jnp.dot(rows_all[r], up_full[:, at], preferred_element_type=f32)
            linear = linear * up_scale_ref[:, span(unit_base + j * up_tile, up_tile)]
            hidden[r, :, at] = jnp.square(jnp.maximum(linear, 0.0)).astype(bf16)

    up_product(0)
    for k in range(2):
        for i in range(steps):
            forward(k, i).wait_recv()
        up_product(k + 1)

    @pl.when(jnp.logical_not(inner))
    def _():
        pass_on(1, zl)

    @pl.when(inner)
    def _():
        pass_on(1, 1 - zl)


    pieces = [(g, same, late) for g in range(2) for same in range(2) for late in range(2)]

    def bit(i):
        g, same, late = pieces[i]
        if g == 0 or same == 0:
            return late
        return zl if late == 0 else 1 - zl

    def place(i):
        g, same, _ = pieces[i]
        n = 2 * same + bit(i)
        return 4 * g + n, n

    def columns(i):
        g, same, _ = pieces[i]
        return line_of(g, bit(i)), y if same == 0 else 1 - y

    def owner(i):
        return (zh if pieces[i][0] == 0 else 1 - zh) == core

    def term_copy(i, k):
        at, n = place(i)
        src, dst = (terms.at[at, 3], terms_in.at[n, 3]) if k else (terms.at[at, 0:3], terms_in.at[n, 0:3])
        return remote(src, dst, term_send.at[n, k], term_recv.at[n, k], pair)

    def routes(i):
        return (2, beside_z, 1, beside_x) if i in (3, 4, 5) else (1, beside_x, 2, beside_z)

    def cross_copy(i, k):
        at, n = place(i)
        slot, to, _, _ = routes(i)
        src = terms.at[at, 3 if k else slot]
        return remote(src, cross_in.at[n, k], cross_send.at[n, k], cross_recv.at[n, k], {"fs": to})

    def line_copy(i):
        at, n = place(i)
        _, _, slot, to = routes(i)
        return remote(terms.at[at, slot], line_in.at[n], line_send.at[n], line_recv.at[n], {"fs": to})

    arrived = set()

    def product_step(i, k):
        g, same, _ = pieces[i]
        if same == 1 and i not in arrived:
            beside(1, g, bit(i)).wait_recv()
        arrived.add(i)
        at, _ = place(i)
        q, yy = columns(i)

        def product(r):
            terms[at, r] = jnp.dot(hidden[r], down_full[:, slab_at(q, yy)], preferred_element_type=f32).astype(bf16)

        if k == 0:
            pl.loop(0, 3)(product)
        else:
            product(3)

        @pl.when(jnp.logical_not(owner(i)))
        def _():
            term_copy(i, k).start()

    def add_step(i, k):
        at, n = place(i)

        @pl.when(owner(i))
        def _():
            term_copy(i, k).wait_recv()

            def add(r):
                @pl.loop(0, rows // fine)
                def _(c):
                    these = span(c * fine, fine, fine)
                    terms[at, r, these, :] = (
                        terms[at, r, these, :].astype(f32) + terms_in[n, r, these, :].astype(f32)
                    ).astype(bf16)

            first, _, second, _ = routes(i)
            if k == 1:
                add(3)
                cross_copy(i, 1).start()
            else:
                add(first)
                cross_copy(i, 0).start()
                add(second)
                add(0)

    def cross_step(i):
        at, n = place(i)

        @pl.when(owner(i))
        def _():
            cross_copy(i, 1).wait_recv()
            slot = routes(i)[2]

            @pl.loop(0, rows // fine)
            def _(c):
                these = span(c * fine, fine, fine)
                terms[at, slot, these, :] = (
                    terms[at, slot, these, :].astype(f32) + cross_in[n, 1, these, :].astype(f32)
                ).astype(bf16)

            line_copy(i).start()
            cross_copy(i, 0).wait_recv()

    def line_step(i):
        at, n = place(i)
        q, yy = columns(i)

        @pl.when(owner(i))
        def _():
            line_copy(i).wait_recv()
            out_at = slab_at(q % 2, yy)

            @pl.loop(0, rows // fine)
            def _(c):
                these = span(c * fine, fine, fine)
                total = terms[at, 0, these, :].astype(f32) + cross_in[n, 0, these, :].astype(f32)
                total = total + line_in[n, these, :].astype(f32)
                out_ref[these, out_at] = (middle[these, slab_at(q, yy)].astype(f32) + total).astype(bf16)

    def far_step(i):
        @pl.when(jnp.logical_not(inner))
        def _():
            pass_on(1, 1 - zl)

    def run_tail(names):
        kinds = dict(
            p=lambda i: (product_step(i, 1), product_step(i, 0)),
            q=lambda i: product_step(i, 0),
            r=lambda i: product_step(i, 1),
            a=lambda i: (add_step(i, 1), add_step(i, 0)),
            b=lambda i: add_step(i, 0),
            d=lambda i: add_step(i, 1),
            c=cross_step,
            l=line_step,
            f=far_step,
        )
        for name in names:
            kinds[name[0]](int(name[1]))

    run_tail(sizes["early"])
    for i in range(steps):
        row_copy(2, i).wait_recv()
        forward(2, i).start()
    for i in range(steps):
        forward(2, i).wait_recv()
    up_product(3)
    run_tail(sizes["late"])

    for copy in half_copies + sum_copies + part_copies + share_copies + middle_copies:
        copy.wait_send()
    for a in range(2):
        for k in range(3):
            swap(a, k).wait_send()
        for b in range(2):
            across(a, b).wait_send()
            for g in range(2):
                beside(a, g, b).wait_send()
    for q in range(LINES):
        for away in range(2):
            for copy in gate_cross(q, y, away):
                copy.wait_send()
    for side, step in ((0, 1), (1, -1)):
        for d in range(LINES):
            q = z - step * d

            @pl.when((q >= 0) & (q < LINES) & (z + step >= 0) & (z + step < LINES))
            def _(q=q, side=side, step=step):
                for away in range(2):
                    for copy in gate_line(q, side, step, away):
                        copy.wait_send()

    for k in range(3):
        for i in range(steps):
            row_copy(k, i).wait_send()
            forward(k, i).wait_send()
    for i in range(4):
        for k in range(2):
            cross_copy(i, k).wait_send()
        line_copy(i).wait_send()
        for k in range(2):
            term_copy(i, k).wait_send()


def fused_shards(fs, tokens, mixer_gain, w_content, w_spatial, content_scale, spatial_scale, spatial_gain,
                 block_mixing, block_bias, w_project, project_scale, channel_gain, w_up, up_scale, w_down, down_scale):
    rows, half = tokens.shape
    width = 2 * half
    channels = w_content.shape[1]
    share_width = channels // 2
    hidden_units = w_up.shape[1]
    units = hidden_units // 4
    depth = w_up.shape[0]
    slab = 2 * depth
    steps = rows // block_mixing.shape[1]
    bf16, f32 = jnp.bfloat16, jnp.float32
    early = [
        "q0", "q2", "b0", "b2",
    ]
    late = [
        "r0", "r2", "d0", "f1", "p4", "d2", "p5", "a4", "p1", "a5", "p6", "a1", "p3", "a6", "c0", "a3", "c2",
        "p7", "a7", "c4", "c5", "c1", "c6", "c3", "c7", "l0", "l2", "l4", "l5", "l1", "l3", "l6", "l7",
    ]
    sizes = dict(fine=64, tile=256, up_tile=256, early=early, late=late)
    vmem = pltpu.VMEM
    dma = pltpu.SemaphoreType.DMA
    row = lambda a: a.reshape(1, -1)
    sems = [(3,), (2,), None, None, (2, 3), (2, 2), (2, 2, 2), (3,), (2,), (steps,), (steps,), (3, steps), (3, steps),
            (4, 2), (4, 2), (4,)]
    pairs = []
    for shape in sems:
        if shape is not None:
            pairs += [dma(shape), dma(shape)]
        elif len(pairs) == 4:
            pairs += [dma((2, 2, 2, LINES)), dma((2, 2, LINES))]
        else:
            pairs += [dma((2, 2, LINES)), dma((2, 2, LINES))]
    return pl.pallas_call(
        functools.partial(layer_kernel, sizes),
        out_shape=jax.ShapeDtypeStruct((rows, half), bf16),
        in_specs=[
            pl.BlockSpec(memory_space=pl.ANY if i in (12, 14) else vmem) for i in range(16)
        ],
        out_specs=pl.BlockSpec(memory_space=vmem),
        scratch_shapes=[
            vmem((depth, hidden_units), f32),
            vmem((hidden_units, depth), f32),
            dma((2,)),
            vmem((2, rows, width), bf16),
            vmem((2, rows, width), bf16),
            vmem((width, 2 * share_width), bf16),
            vmem((share_width, width), bf16),
            vmem((depth, 2 * share_width), bf16),
            vmem((share_width, depth), bf16),
            vmem((depth, hidden_units), bf16),
            vmem((hidden_units, depth), bf16),
            vmem((width, units), bf16),
            vmem((units, width), bf16),
            vmem((2, rows, share_width), f32),
            vmem((2, rows, share_width), f32),
            vmem((2, rows, share_width), bf16),
            vmem((8, 128), f32),
            vmem((3, 8, 128), f32),
            vmem((2, rows, width), bf16),
            vmem((2, rows, half), bf16),
            vmem((rows, half), bf16),
            vmem((rows, half), bf16),
            vmem((rows, width), bf16),
            vmem((4, rows, width), bf16),
            vmem((4, rows, units), bf16),
            vmem((8, 4, rows, slab), bf16),
            vmem((4, 4, rows, slab), bf16),
            vmem((4, 2, rows, slab), bf16),
            vmem((4, rows, slab), bf16),
        ] + pairs,
        compiler_params=pltpu.CompilerParams(
            collective_id=0, has_side_effects=True, vmem_limit_bytes=VMEM_LIMIT
        ),
    )(tokens, row(mixer_gain), w_content, w_spatial, row(content_scale), row(spatial_scale), row(spatial_gain),
      block_mixing, block_bias, w_project, row(project_scale), row(channel_gain), w_up, row(up_scale), w_down,
      row(down_scale))


VMEM_LIMIT = 67043328


def solution(mesh):
    fs, tp = mesh.shape["fs"], mesh.shape["tp"]
    if tp == 2 and fs == LINES * PLANE:
        body = functools.partial(fused_shards, fs)
    else:
        body = shards
    return jax.shard_map(
        body,
        mesh=mesh,
        in_specs=(
            P("fs", "tp"),
            P(),
            P("fs", "tp"),
            P("fs", "tp"),
            P("tp"),
            P("tp"),
            P("tp"),
            P("tp", None, None),
            P("tp", None),
            P("tp", "fs"),
            P("fs"),
            P(),
            P("fs", "tp"),
            P("tp"),
            P("tp", "fs"),
            P("fs"),
        ),
        out_specs=P("fs", "tp"),
        check_vma=False,
    )
```

```python
import functools

import jax
import jax.numpy as jnp
from jax import lax
from jax.experimental import pallas as pl
from jax.experimental.pallas import tpu as pltpu
from jax.sharding import PartitionSpec as P

EPSILON = 1e-06


def normalize_rows(token_rows, gain_vector):
    values = token_rows.astype(jnp.float32)
    scaled = values * lax.rsqrt(jnp.mean(values * values, axis=-1, keepdims=True) + EPSILON)
    return (scaled * gain_vector).astype(jnp.bfloat16)


def shards(
    tokens,
    mixer_gain,
    w_content,
    w_spatial,
    content_scale,
    spatial_scale,
    spatial_gain,
    block_mixing,
    block_bias,
    w_project,
    project_scale,
    channel_gain,
    w_up,
    up_scale,
    w_down,
    down_scale,
):
    content_weight = w_content.astype(jnp.bfloat16)
    spatial_weight = w_spatial.astype(jnp.bfloat16)
    project_weight = w_project.astype(jnp.bfloat16)
    up_weight = w_up.astype(jnp.bfloat16)
    down_weight = w_down.astype(jnp.bfloat16)
    project_full, down_full = (
        lax.all_gather(project_scale, "fs", axis=0, tiled=True),
        lax.all_gather(down_scale, "fs", axis=0, tiled=True),
    )
    gathered_rows = lax.all_gather(tokens, "tp", axis=1, tiled=True)
    normed = normalize_rows(gathered_rows, mixer_gain)
    row_count = gathered_rows.shape[0]
    content_full, spatial_full, project_cols = (
        lax.all_gather(content_weight, "fs", axis=0, tiled=True),
        lax.all_gather(spatial_weight, "fs", axis=0, tiled=True),
        lax.all_gather(project_weight, "fs", axis=1, tiled=True),
    )
    content_linear = jnp.dot(normed, content_full, preferred_element_type=jnp.float32)
    spatial_linear = jnp.dot(normed, spatial_full, preferred_element_type=jnp.float32)
    content = jax.nn.gelu(content_linear * content_scale)
    spatial = jax.nn.gelu(spatial_linear * spatial_scale)
    square_sums = lax.psum(jnp.sum(spatial * spatial, axis=1), "tp")
    total_width = spatial.shape[1] * lax.axis_size("tp")
    spatial_norm = (
        spatial * lax.rsqrt(square_sums / total_width + EPSILON)[:, None] * spatial_gain
    ).astype(jnp.bfloat16)
    groups_here = block_mixing.shape[0]
    block_size = block_mixing.shape[1]
    group_width = spatial_norm.shape[1] // groups_here
    causal_mask = jnp.tril(jnp.ones((block_size, block_size), dtype=bool))
    mixing_weights = jnp.where(causal_mask[None, :, :], block_mixing, jnp.zeros_like(block_mixing))
    grouped = spatial_norm.reshape(row_count // block_size, block_size, groups_here, group_width)
    mixed_block = (
        jnp.einsum("gts,nsgc->ntgc", mixing_weights, grouped, preferred_element_type=jnp.float32)
        + block_bias.T[None, :, :, None]
    )
    gated = (content * mixed_block.reshape(row_count, spatial_norm.shape[1])).astype(jnp.bfloat16)
    mixer_terms = jnp.dot(gated, project_cols, preferred_element_type=jnp.float32) * project_full
    mixer_sum = lax.psum_scatter(
        mixer_terms.astype(jnp.bfloat16), "tp", scatter_dimension=1, tiled=True
    ).astype(jnp.float32)
    middle = (tokens.astype(jnp.float32) + mixer_sum).astype(jnp.bfloat16)
    middle_rows = lax.all_gather(middle, "tp", axis=1, tiled=True)
    channel_normed = normalize_rows(middle_rows, channel_gain)
    up_full, down_cols = (
        lax.all_gather(up_weight, "fs", axis=0, tiled=True),
        lax.all_gather(down_weight, "fs", axis=1, tiled=True),
    )
    up_linear = jnp.dot(channel_normed, up_full, preferred_element_type=jnp.float32)
    hidden = jnp.square(jax.nn.relu(up_linear * up_scale)).astype(jnp.bfloat16)
    channel_terms = jnp.dot(hidden, down_cols, preferred_element_type=jnp.float32) * down_full
    channel_sum = lax.psum_scatter(
        channel_terms.astype(jnp.bfloat16), "tp", scatter_dimension=1, tiled=True
    ).astype(jnp.float32)
    return (middle.astype(jnp.float32) + channel_sum).astype(jnp.bfloat16)


LINES = 4
PLANE = 4
MESH = pl.DeviceIdType.MESH


def layer_kernel(
    sizes,
    tokens_hbm,
    mixer_gain_hbm,
    content_hbm,
    spatial_hbm,
    content_scale_hbm,
    spatial_scale_hbm,
    spatial_gain_hbm,
    mixing_hbm,
    bias_hbm,
    project_hbm,
    project_scale_hbm,
    channel_gain_hbm,
    up_hbm,
    up_scale_hbm,
    down_hbm,
    down_scale_hbm,
    out_ref,
    tokens_ref,
    mixer_gain_ref,
    content_ref,
    spatial_ref,
    content_scale_ref,
    spatial_scale_ref,
    spatial_gain_ref,
    mixing_ref,
    bias_ref,
    project_ref,
    project_scale_ref,
    channel_gain_ref,
    up_ref,
    up_scale_ref,
    down_ref,
    down_scale_ref,
    load_sem,
    token_rows,
    normed,
    gate_weights,
    project_full,
    gate_other,
    project_other,
    up_own,
    down_own,
    up_full,
    down_full,
    content_buf,
    spatial_buf,
    gated,
    sums,
    sums_in,
    part,
    part_in,
    share,
    share_in,
    middle,
    rows_all,
    hidden,
    terms,
    terms_in,
    cross_in,
    line_in,
    token_send,
    token_recv,
    half_send,
    half_recv,
    gate_line_send,
    gate_line_recv,
    gate_send,
    gate_recv,
    swap_send,
    swap_recv,
    across_send,
    across_recv,
    beside_send,
    beside_recv,
    sum_send,
    sum_recv,
    part_send,
    part_recv,
    share_send,
    share_recv,
    middle_send,
    middle_recv,
    row_send,
    row_recv,
    fwd_send,
    fwd_recv,
    term_send,
    term_recv,
    cross_send,
    cross_recv,
    line_send,
    line_recv,
):
    rows, half = tokens_ref.shape
    width = 2 * half
    depth = content_ref.shape[0]
    channels = content_ref.shape[1]
    share_width = channels // 2
    units = up_full.shape[1]
    slab = 2 * depth
    fine = sizes["fine"]
    tile = sizes["tile"]
    groups, block_size = mixing_ref.shape[0], mixing_ref.shape[1]
    blocks = rows // block_size
    steps = rows // block_size
    me = lax.axis_index("fs")
    core = lax.axis_index("tp")
    z = me // PLANE
    p = me % PLANE
    y = p // 2
    x = p % 2
    zh = z // 2
    zl = z % 2
    other = 1 - core
    f32, bf16 = jnp.float32, jnp.bfloat16

    def span(start, size, by=128):
        return pl.ds(pl.multiple_of(start, by), size)

    beside_x = me + 1 - 2 * x
    beside_y = me + 2 - 4 * y
    beside_z = me + PLANE * (1 - 2 * zl)
    corner = beside_z + 1 - 2 * x
    far_z = me + 2 * PLANE * (1 - 2 * zh)
    inner = (z > 0) & (z < LINES - 1)
    pair = {"tp": other}
    mine = span(core * half, half)

    def remote(src, dst, send, recv, where):
        return pltpu.make_async_remote_copy(
            src_ref=src, dst_ref=dst, send_sem=send, recv_sem=recv, device_id=where, device_id_type=MESH
        )

    staged = [
        (content_hbm, content_ref),
        (spatial_hbm, spatial_ref),
        (project_hbm, project_ref),
        (project_scale_hbm, project_scale_ref),
        (tokens_hbm, tokens_ref),
        (up_hbm, up_ref),
        (down_hbm, down_ref),
        (down_scale_hbm, down_scale_ref),
        (mixer_gain_hbm, mixer_gain_ref),
        (content_scale_hbm, content_scale_ref),
        (spatial_scale_hbm, spatial_scale_ref),
        (spatial_gain_hbm, spatial_gain_ref),
        (mixing_hbm, mixing_ref),
        (bias_hbm, bias_ref),
        (channel_gain_hbm, channel_gain_ref),
        (up_scale_hbm, up_scale_ref),
    ]
    loads = [pltpu.make_async_copy(src, dst, load_sem.at[i]) for i, (src, dst) in enumerate(staged)]
    for load in loads:
        load.start()
    barrier = pltpu.get_barrier_semaphore()
    friends = [{"fs": i} for i in (beside_x, beside_y, beside_z, corner, far_z)]
    friends += [pair, {"fs": beside_x, "tp": other}]
    for friend in friends:
        pl.semaphore_signal(barrier, inc=1, device_id=friend, device_id_type=MESH)

    @pl.when(inner)
    def _():
        pl.semaphore_signal(
            barrier, inc=1, device_id={"fs": me + PLANE * (2 * zl - 1)}, device_id_type=MESH
        )

    own_channels = span(x * share_width, share_width)
    own_depth = span(me * depth, depth)

    def halves(channel_half, weights, project):
        at = span(channel_half * share_width, share_width)
        weights[:, pl.ds(0, share_width)] = content_ref[:, at].astype(bf16)
        weights[:, pl.ds(share_width, share_width)] = spatial_ref[:, at].astype(bf16)
        project[...] = (project_ref[at, :] * project_scale_ref[...]).astype(bf16)

    for load in loads[:4]:
        load.wait()
    halves(1 - x, gate_other, project_other)
    halves(x, gate_weights.at[own_depth, :], project_full.at[:, own_depth])
    loads[4].wait()
    token_rows[0, :, mine] = tokens_ref[...]
    pl.semaphore_wait(barrier, len(friends) + inner.astype(jnp.int32))

    def slab_at(q, yy):
        return span((q * PLANE + yy * 2) * depth, slab)

    def gate_refs(q, yy, away):
        at = span((q * PLANE + yy * 2 + (1 - x if away else x)) * depth, depth)
        return gate_weights.at[at, :], project_full.at[:, at]

    def gate_line(q, side, step, away):
        refs = gate_refs(q, y, away)
        return [
            remote(
                refs[a], refs[a], gate_line_send.at[a, away, side, q], gate_line_recv.at[a, away, q],
                {"fs": me + step * PLANE},
            )
            for a in range(2)
        ]

    def gate_cross(q, yy, away):
        refs = gate_refs(q, yy, away)
        return [
            remote(refs[a], refs[a], gate_send.at[a, away, q], gate_recv.at[a, away, q], {"fs": beside_y})
            for a in range(2)
        ]

    def start_gate(away):
        for side, step in ((0, 1), (1, -1)):

            @pl.when((z + step >= 0) & (z + step < LINES))
            def _(side=side, step=step):
                for copy in gate_line(z, side, step, away):
                    copy.start()

        for copy in gate_cross(z, y, away):
            copy.start()

    half_copies = [
        remote(gate_other, gate_weights.at[own_depth, :], half_send.at[0], half_recv.at[0], {"fs": beside_x}),
        remote(project_other, project_full.at[:, own_depth], half_send.at[1], half_recv.at[1], {"fs": beside_x}),
    ]

    swap_to = (beside_x, beside_z, corner)
    swap_part = (2 * zl + 1 - x, 2 * (1 - zl) + x, 2 * (1 - zl) + 1 - x)

    def swap(a, k):
        theirs = span(swap_part[k] * units, units)
        src = up_own.at[:, theirs] if a == 0 else down_own.at[theirs, :]
        dst = up_full.at[own_depth, :] if a == 0 else down_full.at[:, own_depth]
        return remote(src, dst, swap_send.at[a, k], swap_recv.at[a, k], {"fs": swap_to[k]})

    def ff_ref(a, q, yy):
        return up_full.at[slab_at(q, yy), :] if a == 0 else down_full.at[:, slab_at(q, yy)]

    def line_of(g, b):
        return 2 * (zh if g == 0 else 1 - zh) + b

    def across(a, b):
        ref = ff_ref(a, line_of(0, b), y)
        return remote(ref, ref, across_send.at[a, b], across_recv.at[a, b], {"fs": far_z})

    def beside(a, g, b):
        ref = ff_ref(a, line_of(g, b), y)
        return remote(ref, ref, beside_send.at[a, g, b], beside_recv.at[a, g, b], {"fs": beside_y})

    def relay_gate(d, away):
        for side, step in ((0, 1), (1, -1)):
            q = z - step * d

            @pl.when((q >= 0) & (q < LINES))
            def _(q=q, side=side, step=step):
                for copy in gate_line(q, side, step, away):
                    copy.wait_recv()

                @pl.when((z + step >= 0) & (z + step < LINES))
                def _():
                    for copy in gate_line(q, side, step, away):
                        copy.start()

                for copy in gate_cross(q, y, away):
                    copy.start()

    for copy in half_copies:
        copy.start()
    start_gate(0)
    token_pair = remote(tokens_ref, token_rows.at[0, :, mine], token_send.at[0], token_recv.at[0], pair)
    token_pair.start()
    for load in loads[5:]:
        load.wait()

    @pl.loop(0, up_own.shape[1] // units)
    def _(j):
        up_own[:, span(j * units, units)] = up_ref[:, span(j * units, units)].astype(bf16)

    quarter = span((2 * zl + x) * units, units)
    swap(0, 0).start()
    token_cross = remote(
        tokens_ref, token_rows.at[1, :, mine], token_send.at[1], token_recv.at[1], {"fs": beside_x}
    )
    token_cross.start()
    up_full[own_depth, :] = up_ref[:, quarter].astype(bf16)

    @pl.loop(0, up_own.shape[1] // units)
    def _(j):
        down_own[span(j * units, units), :] = (
            down_ref[span(j * units, units), :] * down_scale_ref[...]
        ).astype(bf16)

    down_full[:, own_depth] = (down_ref[quarter, :] * down_scale_ref[...]).astype(bf16)

    for copy in half_copies:
        copy.wait_recv()
    start_gate(1)

    @pl.when(jnp.logical_not(inner))
    def _():
        swap(0, 1).start()
        swap(0, 2).start()

    def normalize(source, gain_ref, target, first, count):
        @pl.loop(0, count // fine)
        def _(i):
            these = span(first + i * fine, fine, fine)
            values = source[these, :].astype(f32)
            scaled = values * lax.rsqrt(jnp.mean(values * values, axis=-1, keepdims=True) + EPSILON)
            target[these, :] = (scaled * gain_ref[...]).astype(bf16)

    token_pair.wait()
    normalize(token_rows.at[0], mixer_gain_ref, normed.at[0], 0, rows)
    relay_gate(1, 0)
    relay_gate(1, 1)
    swap(0, 0).wait_recv()
    relay_gate(2, 0)
    relay_gate(2, 1)

    @pl.when(inner)
    def _():
        swap(0, 1).start()
        swap(0, 2).start()

    @pl.when(jnp.logical_not(inner))
    def _():
        across(0, zl).start()

    swap(1, 0).start()
    relay_gate(3, 0)
    relay_gate(3, 1)
    beside(0, 0, zl).start()
    token_cross.wait()

    @pl.when(inner)
    def _():
        across(0, zl).start()


    token_forward = remote(
        token_rows.at[1, :, mine], token_rows.at[1, :, mine], token_send.at[2], token_recv.at[2], pair
    )
    token_forward.start()
    token_forward.wait()
    normalize(token_rows.at[1], mixer_gain_ref, normed.at[1], 0, rows)

    def finish_up_swap():
        swap(0, 1).wait_recv()
        swap(0, 2).wait_recv()
        across(0, 1 - zl).start()
        beside(0, 0, 1 - zl).start()

    @pl.when(inner)
    def _():
        finish_up_swap()

    swap(1, 1).start()
    swap(1, 2).start()
    swap(1, 0).wait_recv()

    @pl.when(jnp.logical_not(inner))
    def _():
        across(1, zl).start()

    beside(1, 0, zl).start()

    def finish_down_swap():
        swap(1, 1).wait_recv()
        swap(1, 2).wait_recv()
        across(1, 1 - zl).start()

    for q in range(LINES):
        for away in range(2):
            for copy in gate_cross(q, 1 - y, away):
                copy.wait_recv()

    @pl.loop(0, 2)
    def _(s):
        linear = jnp.dot(normed[s], gate_weights[:, pl.ds(share_width, share_width)], preferred_element_type=f32)
        spatial_buf[s] = jax.nn.gelu(linear * spatial_scale_ref[:, own_channels])

    sums[...] = jnp.zeros_like(sums)
    for s in range(2):
        for n in range(blocks):
            values = spatial_buf[s, pl.ds(n * block_size, block_size), :]
            total = jnp.sum(values * values, axis=1, keepdims=True)
            sums[pl.ds(s * blocks + n, 1), :] = jnp.broadcast_to(total, (block_size, block_size)).T[:1, :]
    sum_to = (pair, {"fs": beside_x}, {"fs": beside_x, "tp": other})
    sum_copies = [remote(sums, sums_in.at[k], sum_send.at[k], sum_recv.at[k], sum_to[k]) for k in range(3)]
    for copy in sum_copies:
        copy.start()

    @pl.loop(0, 2)
    def _(s):
        linear = jnp.dot(normed[s], gate_weights[:, pl.ds(0, share_width)], preferred_element_type=f32)
        content_buf[s] = jax.nn.gelu(linear * content_scale_ref[:, own_channels])

    for copy in sum_copies:
        copy.wait_recv()

    causal = lax.broadcasted_iota(jnp.int32, (block_size, block_size), 0) >= lax.broadcasted_iota(
        jnp.int32, (block_size, block_size), 1
    )
    own_groups = groups // 2
    group_width = channels // groups
    part_copies = [
        remote(
            part.at[s, :, span(other * half, half)], part_in.at[s], part_send.at[s], part_recv.at[s], pair
        )
        for s in range(2)
    ]
    for s in (1, 0):
        for n in range(blocks):
            these = pl.ds(n * block_size, block_size)
            here, there = pl.ds(s * blocks + n, 1), pl.ds((1 - s) * blocks + n, 1)
            total = (sums[here, :] + sums_in[0, here, :]) + (sums_in[1, there, :] + sums_in[2, there, :])
            scale = lax.rsqrt(total / (2 * channels) + EPSILON)
            scale = jnp.broadcast_to(scale, (block_size, block_size)).T[:, :1]
            for g in range(own_groups):
                group = x * own_groups + g
                weights = jnp.where(causal, mixing_ref[group].astype(f32), 0.0).astype(bf16)
                bias = jnp.broadcast_to(bias_ref[pl.ds(group, 1), :], (block_size, block_size)).T[:, :1]
                at = pl.ds(g * group_width, group_width)
                gain = spatial_gain_ref[:, span(group * group_width, group_width)]
                spatial_norm = (spatial_buf[s, these, at] * scale * gain).astype(bf16)
                mixed = jnp.dot(weights, spatial_norm, preferred_element_type=f32) + bias
                gated[s, these, at] = (content_buf[s, these, at] * mixed).astype(bf16)

        @pl.loop(0, width // (2 * tile))
        def _(j, s=s):
            at = span(j * 2 * tile, 2 * tile)
            part[s, :, at] = jnp.dot(gated[s], project_full[:, at], preferred_element_type=f32).astype(bf16)

        part_copies[s].start()

    def step_rows(i):
        return pl.ds(i * block_size, block_size)

    share_copies = [
        remote(
            share.at[step_rows(i), :], share_in.at[step_rows(i), :], share_send.at[i], share_recv.at[i],
            {"fs": beside_x},
        )
        for i in range(steps)
    ]
    part_copies[1].wait_recv()
    for i in range(steps):
        these = step_rows(i)
        share[these, :] = (part[1, these, mine].astype(f32) + part_in[1, these, :].astype(f32)).astype(bf16)
        share_copies[i].start()
    part_copies[0].wait_recv()

    middle_copies = [
        remote(
            middle.at[step_rows(i), mine], middle.at[step_rows(i), mine], middle_send.at[i], middle_recv.at[i], pair
        )
        for i in range(steps)
    ]

    def row_copy(k, i):
        src = rows_all.at[2 if k == 2 else 0, step_rows(i), mine]
        dst = rows_all.at[k + 1, step_rows(i), mine]
        return remote(src, dst, row_send.at[k, i], row_recv.at[k, i], {"fs": beside_z if k == 1 else beside_x})

    def forward(k, i):
        ref = rows_all.at[k + 1, step_rows(i), mine]
        return remote(ref, ref, fwd_send.at[k, i], fwd_recv.at[k, i], pair)

    @pl.when(jnp.logical_not(inner))
    def _():
        finish_up_swap()

    for i in range(steps):
        these = step_rows(i)
        share_copies[i].wait_recv()
        total = part[0, these, mine].astype(f32) + part_in[0, these, :].astype(f32)
        total = total + share_in[these, :].astype(f32)
        middle[these, mine] = (tokens_ref[these, :].astype(f32) + total).astype(bf16)
        middle_copies[i].start()
        middle_copies[i].wait_recv()
        normalize(middle, channel_gain_ref, rows_all.at[0], i * block_size, block_size)
        row_copy(1, i).start()
        row_copy(0, i).start()
        if i == steps - 2:
            across(0, zl).wait_recv()
            beside(0, 1, zl).start()

    def pass_on(a, b):
        across(a, b).wait_recv()
        beside(a, 1, b).start()

    @pl.when(jnp.logical_not(inner))
    def _():
        pass_on(0, 1 - zl)

    for i in range(steps):
        row_copy(1, i).wait_recv()
        row_copy(2, i).start()
        forward(1, i).start()
        if i == 0:

            @pl.when(jnp.logical_not(inner))
            def _():
                finish_down_swap()

            @pl.when(inner)
            def _():
                pass_on(0, 1 - zl)

        if i == steps - 2:

            @pl.when(inner)
            def _():
                across(1, zl).start()

    @pl.when(inner)
    def _():
        finish_down_swap()

    beside(1, 0, 1 - zl).start()

    @pl.when(inner)
    def _():
        pass_on(1, zl)

    for i in range(steps):
        row_copy(0, i).wait_recv()
        forward(0, i).start()
    for g in range(2):
        for b in range(2):
            beside(0, g, b).wait_recv()

    up_tile = sizes["up_tile"]
    unit_base = (2 * zl + x) * units

    def up_product(r):
        @pl.loop(0, units // up_tile)
        def _(j):
            at = span(j * up_tile, up_tile)
            linear = jnp.dot(rows_all[r], up_full[:, at], preferred_element_type=f32)
            linear = linear * up_scale_ref[:, span(unit_base + j * up_tile, up_tile)]
            hidden[r, :, at] = jnp.square(jnp.maximum(linear, 0.0)).astype(bf16)

    up_product(0)
    for k in range(2):
        for i in range(steps):
            forward(k, i).wait_recv()
        up_product(k + 1)

    @pl.when(jnp.logical_not(inner))
    def _():
        pass_on(1, zl)

    @pl.when(inner)
    def _():
        pass_on(1, 1 - zl)


    pieces = [(g, same, late) for g in range(2) for same in range(2) for late in range(2)]

    def bit(i):
        g, same, late = pieces[i]
        if g == 0 or same == 0:
            return late
        return zl if late == 0 else 1 - zl

    def place(i):
        g, same, _ = pieces[i]
        n = 2 * same + bit(i)
        return 4 * g + n, n

    def columns(i):
        g, same, _ = pieces[i]
        return line_of(g, bit(i)), y if same == 0 else 1 - y

    def owner(i):
        return (zh if pieces[i][0] == 0 else 1 - zh) == core

    def term_copy(i, k):
        at, n = place(i)
        src, dst = (terms.at[at, 3], terms_in.at[n, 3]) if k else (terms.at[at, 0:3], terms_in.at[n, 0:3])
        return remote(src, dst, term_send.at[n, k], term_recv.at[n, k], pair)

    def routes(i):
        return (2, beside_z, 1, beside_x) if i in (3, 4, 5) else (1, beside_x, 2, beside_z)

    def cross_copy(i, k):
        at, n = place(i)
        slot, to, _, _ = routes(i)
        src = terms.at[at, 3 if k else slot]
        return remote(src, cross_in.at[n, k], cross_send.at[n, k], cross_recv.at[n, k], {"fs": to})

    def line_copy(i):
        at, n = place(i)
        _, _, slot, to = routes(i)
        return remote(terms.at[at, slot], line_in.at[n], line_send.at[n], line_recv.at[n], {"fs": to})

    arrived = set()

    def product_step(i, k):
        g, same, _ = pieces[i]
        if same == 1 and i not in arrived:
            beside(1, g, bit(i)).wait_recv()
        arrived.add(i)
        at, _ = place(i)
        q, yy = columns(i)

        def product(r):
            terms[at, r] = jnp.dot(hidden[r], down_full[:, slab_at(q, yy)], preferred_element_type=f32).astype(bf16)

        if k == 0:
            pl.loop(0, 3)(product)
        else:
            product(3)

        @pl.when(jnp.logical_not(owner(i)))
        def _():
            term_copy(i, k).start()

    def add_step(i, k):
        at, n = place(i)

        @pl.when(owner(i))
        def _():
            term_copy(i, k).wait_recv()

            def add(r):
                @pl.loop(0, rows // fine)
                def _(c):
                    these = span(c * fine, fine, fine)
                    terms[at, r, these, :] = (
                        terms[at, r, these, :].astype(f32) + terms_in[n, r, these, :].astype(f32)
                    ).astype(bf16)

            first, _, second, _ = routes(i)
            if k == 1:
                add(3)
                cross_copy(i, 1).start()
            else:
                add(first)
                cross_copy(i, 0).start()
                add(second)
                add(0)

    def cross_step(i):
        at, n = place(i)

        @pl.when(owner(i))
        def _():
            cross_copy(i, 1).wait_recv()
            slot = routes(i)[2]

            @pl.loop(0, rows // fine)
            def _(c):
                these = span(c * fine, fine, fine)
                terms[at, slot, these, :] = (
                    terms[at, slot, these, :].astype(f32) + cross_in[n, 1, these, :].astype(f32)
                ).astype(bf16)

            line_copy(i).start()
            cross_copy(i, 0).wait_recv()

    def line_step(i):
        at, n = place(i)
        q, yy = columns(i)

        @pl.when(owner(i))
        def _():
            line_copy(i).wait_recv()
            out_at = slab_at(q % 2, yy)

            @pl.loop(0, rows // fine)
            def _(c):
                these = span(c * fine, fine, fine)
                total = terms[at, 0, these, :].astype(f32) + cross_in[n, 0, these, :].astype(f32)
                total = total + line_in[n, these, :].astype(f32)
                out_ref[these, out_at] = (middle[these, slab_at(q, yy)].astype(f32) + total).astype(bf16)

    def far_step(i):
        @pl.when(jnp.logical_not(inner))
        def _():
            pass_on(1, 1 - zl)

    def run_tail(names):
        kinds = dict(
            p=lambda i: (product_step(i, 1), product_step(i, 0)),
            q=lambda i: product_step(i, 0),
            r=lambda i: product_step(i, 1),
            a=lambda i: (add_step(i, 1), add_step(i, 0)),
            b=lambda i: add_step(i, 0),
            d=lambda i: add_step(i, 1),
            c=cross_step,
            l=line_step,
            f=far_step,
        )
        for name in names:
            kinds[name[0]](int(name[1]))

    run_tail(sizes["early"])
    for i in range(steps):
        row_copy(2, i).wait_recv()
        forward(2, i).start()
    for i in range(steps):
        forward(2, i).wait_recv()
    up_product(3)
    run_tail(sizes["late"])

    for copy in half_copies + sum_copies + part_copies + share_copies + middle_copies:
        copy.wait_send()
    for a in range(2):
        for k in range(3):
            swap(a, k).wait_send()
        for b in range(2):
            across(a, b).wait_send()
            for g in range(2):
                beside(a, g, b).wait_send()
    for q in range(LINES):
        for away in range(2):
            for copy in gate_cross(q, y, away):
                copy.wait_send()
    for side, step in ((0, 1), (1, -1)):
        for d in range(LINES):
            q = z - step * d

            @pl.when((q >= 0) & (q < LINES) & (z + step >= 0) & (z + step < LINES))
            def _(q=q, side=side, step=step):
                for away in range(2):
                    for copy in gate_line(q, side, step, away):
                        copy.wait_send()

    for k in range(3):
        for i in range(steps):
            row_copy(k, i).wait_send()
            forward(k, i).wait_send()
    for i in range(4):
        for k in range(2):
            cross_copy(i, k).wait_send()
        line_copy(i).wait_send()
        for k in range(2):
            term_copy(i, k).wait_send()


def fused_shards(fs, tokens, mixer_gain, w_content, w_spatial, content_scale, spatial_scale, spatial_gain,
                 block_mixing, block_bias, w_project, project_scale, channel_gain, w_up, up_scale, w_down, down_scale):
    rows, half = tokens.shape
    width = 2 * half
    channels = w_content.shape[1]
    share_width = channels // 2
    hidden_units = w_up.shape[1]
    units = hidden_units // 4
    depth = w_up.shape[0]
    slab = 2 * depth
    steps = rows // block_mixing.shape[1]
    bf16, f32 = jnp.bfloat16, jnp.float32
    early = [
        "q0", "q2", "b0", "b2",
    ]
    late = [
        "r0", "r2", "d0", "f1", "p4", "d2", "p5", "a4", "p1", "a5", "p6", "a1", "p3", "a6", "c0", "a3", "c2",
        "p7", "a7", "c4", "c5", "c1", "c6", "c3", "c7", "l0", "l2", "l4", "l5", "l1", "l3", "l6", "l7",
    ]
    sizes = dict(fine=64, tile=256, up_tile=256, early=early, late=late)
    vmem = pltpu.VMEM
    dma = pltpu.SemaphoreType.DMA
    row = lambda a: a.reshape(1, -1)
    operands = (
        tokens, row(mixer_gain), w_content, w_spatial, row(content_scale), row(spatial_scale), row(spatial_gain),
        block_mixing, block_bias, w_project, row(project_scale), row(channel_gain), w_up, row(up_scale), w_down,
        row(down_scale),
    )
    sems = [(3,), (2,), None, None, (2, 3), (2, 2), (2, 2, 2), (3,), (2,), (steps,), (steps,), (3, steps), (3, steps),
            (4, 2), (4, 2), (4,)]
    pairs = []
    for shape in sems:
        if shape is not None:
            pairs += [dma(shape), dma(shape)]
        elif len(pairs) == 4:
            pairs += [dma((2, 2, 2, LINES)), dma((2, 2, LINES))]
        else:
            pairs += [dma((2, 2, LINES)), dma((2, 2, LINES))]
    return pl.pallas_call(
        functools.partial(layer_kernel, sizes),
        out_shape=jax.ShapeDtypeStruct((rows, half), bf16),
        in_specs=[
            pl.BlockSpec(memory_space=pl.ANY) for _ in range(16)
        ],
        out_specs=pl.BlockSpec(memory_space=vmem),
        scratch_shapes=[
            *[vmem(a.shape, a.dtype) for a in operands],
            dma((len(operands),)),
            vmem((2, rows, width), bf16),
            vmem((2, rows, width), bf16),
            vmem((width, 2 * share_width), bf16),
            vmem((share_width, width), bf16),
            vmem((depth, 2 * share_width), bf16),
            vmem((share_width, depth), bf16),
            vmem((depth, hidden_units), bf16),
            vmem((hidden_units, depth), bf16),
            vmem((width, units), bf16),
            vmem((units, width), bf16),
            vmem((2, rows, share_width), f32),
            vmem((2, rows, share_width), f32),
            vmem((2, rows, share_width), bf16),
            vmem((8, 128), f32),
            vmem((3, 8, 128), f32),
            vmem((2, rows, width), bf16),
            vmem((2, rows, half), bf16),
            vmem((rows, half), bf16),
            vmem((rows, half), bf16),
            vmem((rows, width), bf16),
            vmem((4, rows, width), bf16),
            vmem((4, rows, units), bf16),
            vmem((8, 4, rows, slab), bf16),
            vmem((4, 4, rows, slab), bf16),
            vmem((4, 2, rows, slab), bf16),
            vmem((4, rows, slab), bf16),
        ] + pairs,
        compiler_params=pltpu.CompilerParams(
            collective_id=0, has_side_effects=True, vmem_limit_bytes=VMEM_LIMIT
        ),
    )(*operands)


VMEM_LIMIT = 67043328


def solution(mesh):
    fs, tp = mesh.shape["fs"], mesh.shape["tp"]
    if tp == 2 and fs == LINES * PLANE:
        body = functools.partial(fused_shards, fs)
    else:
        body = shards
    return jax.shard_map(
        body,
        mesh=mesh,
        in_specs=(
            P("fs", "tp"),
            P(),
            P("fs", "tp"),
            P("fs", "tp"),
            P("tp"),
            P("tp"),
            P("tp"),
            P("tp", None, None),
            P("tp", None),
            P("tp", "fs"),
            P("fs"),
            P(),
            P("fs", "tp"),
            P("tp"),
            P("tp", "fs"),
            P("fs"),
        ),
        out_specs=P("fs", "tp"),
        check_vma=False,
    )
```

```python
import functools

import jax
import jax.numpy as jnp
from jax import lax
from jax.experimental import pallas as pl
from jax.experimental.pallas import tpu as pltpu
from jax.sharding import PartitionSpec as P

EPSILON = 1e-06


def normalize_rows(token_rows, gain_vector):
    values = token_rows.astype(jnp.float32)
    scaled = values * lax.rsqrt(jnp.mean(values * values, axis=-1, keepdims=True) + EPSILON)
    return (scaled * gain_vector).astype(jnp.bfloat16)


def shards(
    tokens,
    mixer_gain,
    w_content,
    w_spatial,
    content_scale,
    spatial_scale,
    spatial_gain,
    block_mixing,
    block_bias,
    w_project,
    project_scale,
    channel_gain,
    w_up,
    up_scale,
    w_down,
    down_scale,
):
    content_weight = w_content.astype(jnp.bfloat16)
    spatial_weight = w_spatial.astype(jnp.bfloat16)
    project_weight = w_project.astype(jnp.bfloat16)
    up_weight = w_up.astype(jnp.bfloat16)
    down_weight = w_down.astype(jnp.bfloat16)
    project_full, down_full = (
        lax.all_gather(project_scale, "fs", axis=0, tiled=True),
        lax.all_gather(down_scale, "fs", axis=0, tiled=True),
    )
    gathered_rows = lax.all_gather(tokens, "tp", axis=1, tiled=True)
    normed = normalize_rows(gathered_rows, mixer_gain)
    row_count = gathered_rows.shape[0]
    content_full, spatial_full, project_cols = (
        lax.all_gather(content_weight, "fs", axis=0, tiled=True),
        lax.all_gather(spatial_weight, "fs", axis=0, tiled=True),
        lax.all_gather(project_weight, "fs", axis=1, tiled=True),
    )
    content_linear = jnp.dot(normed, content_full, preferred_element_type=jnp.float32)
    spatial_linear = jnp.dot(normed, spatial_full, preferred_element_type=jnp.float32)
    content = jax.nn.gelu(content_linear * content_scale)
    spatial = jax.nn.gelu(spatial_linear * spatial_scale)
    square_sums = lax.psum(jnp.sum(spatial * spatial, axis=1), "tp")
    total_width = spatial.shape[1] * lax.axis_size("tp")
    spatial_norm = (
        spatial * lax.rsqrt(square_sums / total_width + EPSILON)[:, None] * spatial_gain
    ).astype(jnp.bfloat16)
    groups_here = block_mixing.shape[0]
    block_size = block_mixing.shape[1]
    group_width = spatial_norm.shape[1] // groups_here
    causal_mask = jnp.tril(jnp.ones((block_size, block_size), dtype=bool))
    mixing_weights = jnp.where(causal_mask[None, :, :], block_mixing, jnp.zeros_like(block_mixing))
    grouped = spatial_norm.reshape(row_count // block_size, block_size, groups_here, group_width)
    mixed_block = (
        jnp.einsum("gts,nsgc->ntgc", mixing_weights, grouped, preferred_element_type=jnp.float32)
        + block_bias.T[None, :, :, None]
    )
    gated = (content * mixed_block.reshape(row_count, spatial_norm.shape[1])).astype(jnp.bfloat16)
    mixer_terms = jnp.dot(gated, project_cols, preferred_element_type=jnp.float32) * project_full
    mixer_sum = lax.psum_scatter(
        mixer_terms.astype(jnp.bfloat16), "tp", scatter_dimension=1, tiled=True
    ).astype(jnp.float32)
    middle = (tokens.astype(jnp.float32) + mixer_sum).astype(jnp.bfloat16)
    middle_rows = lax.all_gather(middle, "tp", axis=1, tiled=True)
    channel_normed = normalize_rows(middle_rows, channel_gain)
    up_full, down_cols = (
        lax.all_gather(up_weight, "fs", axis=0, tiled=True),
        lax.all_gather(down_weight, "fs", axis=1, tiled=True),
    )
    up_linear = jnp.dot(channel_normed, up_full, preferred_element_type=jnp.float32)
    hidden = jnp.square(jax.nn.relu(up_linear * up_scale)).astype(jnp.bfloat16)
    channel_terms = jnp.dot(hidden, down_cols, preferred_element_type=jnp.float32) * down_full
    channel_sum = lax.psum_scatter(
        channel_terms.astype(jnp.bfloat16), "tp", scatter_dimension=1, tiled=True
    ).astype(jnp.float32)
    return (middle.astype(jnp.float32) + channel_sum).astype(jnp.bfloat16)


LINES = 4
PLANE = 4
MESH = pl.DeviceIdType.MESH


def layer_kernel(
    sizes,
    tokens_hbm,
    mixer_gain_hbm,
    content_hbm,
    spatial_hbm,
    content_scale_hbm,
    spatial_scale_hbm,
    spatial_gain_hbm,
    mixing_hbm,
    bias_hbm,
    project_hbm,
    project_scale_hbm,
    channel_gain_hbm,
    up_hbm,
    up_scale_hbm,
    down_hbm,
    down_scale_hbm,
    out_hbm,
    tokens_ref,
    mixer_gain_ref,
    content_ref,
    spatial_ref,
    content_scale_ref,
    spatial_scale_ref,
    spatial_gain_ref,
    mixing_ref,
    bias_ref,
    project_ref,
    project_scale_ref,
    channel_gain_ref,
    up_ref,
    up_scale_ref,
    down_ref,
    down_scale_ref,
    load_sem,
    token_rows,
    normed,
    gate_weights,
    project_full,
    gate_other,
    project_other,
    up_own,
    down_own,
    up_full,
    down_full,
    content_buf,
    spatial_buf,
    gated,
    sums,
    sums_in,
    part,
    part_in,
    share,
    share_in,
    middle,
    rows_all,
    hidden,
    terms,
    terms_in,
    cross_in,
    line_in,
    token_send,
    token_recv,
    half_send,
    half_recv,
    gate_line_send,
    gate_line_recv,
    gate_send,
    gate_recv,
    swap_send,
    swap_recv,
    across_send,
    across_recv,
    beside_send,
    beside_recv,
    sum_send,
    sum_recv,
    part_send,
    part_recv,
    share_send,
    share_recv,
    middle_send,
    middle_recv,
    row_send,
    row_recv,
    fwd_send,
    fwd_recv,
    term_send,
    term_recv,
    cross_send,
    cross_recv,
    line_send,
    line_recv,
    out_ref,
    out_sem,
):
    rows, half = tokens_ref.shape
    width = 2 * half
    depth = content_ref.shape[0]
    channels = content_ref.shape[1]
    share_width = channels // 2
    units = up_full.shape[1]
    slab = 2 * depth
    fine = sizes["fine"]
    tile = sizes["tile"]
    groups, block_size = mixing_ref.shape[0], mixing_ref.shape[1]
    blocks = rows // block_size
    steps = rows // block_size
    me = lax.axis_index("fs")
    core = lax.axis_index("tp")
    z = me // PLANE
    p = me % PLANE
    y = p // 2
    x = p % 2
    zh = z // 2
    zl = z % 2
    other = 1 - core
    f32, bf16 = jnp.float32, jnp.bfloat16

    def span(start, size, by=128):
        return pl.ds(pl.multiple_of(start, by), size)

    beside_x = me + 1 - 2 * x
    beside_y = me + 2 - 4 * y
    beside_z = me + PLANE * (1 - 2 * zl)
    corner = beside_z + 1 - 2 * x
    far_z = me + 2 * PLANE * (1 - 2 * zh)
    inner = (z > 0) & (z < LINES - 1)
    pair = {"tp": other}
    mine = span(core * half, half)

    def remote(src, dst, send, recv, where):
        return pltpu.make_async_remote_copy(
            src_ref=src, dst_ref=dst, send_sem=send, recv_sem=recv, device_id=where, device_id_type=MESH
        )

    staged = [
        (content_hbm, content_ref),
        (spatial_hbm, spatial_ref),
        (project_hbm, project_ref),
        (project_scale_hbm, project_scale_ref),
        (tokens_hbm, tokens_ref),
        (up_hbm, up_ref),
        (down_hbm, down_ref),
        (down_scale_hbm, down_scale_ref),
        (mixer_gain_hbm, mixer_gain_ref),
        (content_scale_hbm, content_scale_ref),
        (spatial_scale_hbm, spatial_scale_ref),
        (spatial_gain_hbm, spatial_gain_ref),
        (mixing_hbm, mixing_ref),
        (bias_hbm, bias_ref),
        (channel_gain_hbm, channel_gain_ref),
        (up_scale_hbm, up_scale_ref),
    ]
    loads = [pltpu.make_async_copy(src, dst, load_sem.at[i]) for i, (src, dst) in enumerate(staged)]
    for load in loads:
        load.start()
    barrier = pltpu.get_barrier_semaphore()
    friends = [{"fs": i} for i in (beside_x, beside_y, beside_z, corner, far_z)]
    friends += [pair, {"fs": beside_x, "tp": other}]
    for friend in friends:
        pl.semaphore_signal(barrier, inc=1, device_id=friend, device_id_type=MESH)

    @pl.when(inner)
    def _():
        pl.semaphore_signal(
            barrier, inc=1, device_id={"fs": me + PLANE * (2 * zl - 1)}, device_id_type=MESH
        )

    own_channels = span(x * share_width, share_width)
    own_depth = span(me * depth, depth)

    def halves(channel_half, weights, project):
        at = span(channel_half * share_width, share_width)
        weights[:, pl.ds(0, share_width)] = content_ref[:, at].astype(bf16)
        weights[:, pl.ds(share_width, share_width)] = spatial_ref[:, at].astype(bf16)
        project[...] = (project_ref[at, :] * project_scale_ref[...]).astype(bf16)

    for load in loads[:4]:
        load.wait()
    halves(1 - x, gate_other, project_other)
    halves(x, gate_weights.at[own_depth, :], project_full.at[:, own_depth])
    loads[4].wait()
    token_rows[0, :, mine] = tokens_ref[...]
    pl.semaphore_wait(barrier, len(friends) + inner.astype(jnp.int32))

    def slab_at(q, yy):
        return span((q * PLANE + yy * 2) * depth, slab)

    def gate_refs(q, yy, away):
        at = span((q * PLANE + yy * 2 + (1 - x if away else x)) * depth, depth)
        return gate_weights.at[at, :], project_full.at[:, at]

    def gate_line(q, side, step, away):
        refs = gate_refs(q, y, away)
        return [
            remote(
                refs[a], refs[a], gate_line_send.at[a, away, side, q], gate_line_recv.at[a, away, q],
                {"fs": me + step * PLANE},
            )
            for a in range(2)
        ]

    def gate_cross(q, yy, away):
        refs = gate_refs(q, yy, away)
        return [
            remote(refs[a], refs[a], gate_send.at[a, away, q], gate_recv.at[a, away, q], {"fs": beside_y})
            for a in range(2)
        ]

    def start_gate(away):
        for side, step in ((0, 1), (1, -1)):

            @pl.when((z + step >= 0) & (z + step < LINES))
            def _(side=side, step=step):
                for copy in gate_line(z, side, step, away):
                    copy.start()

        for copy in gate_cross(z, y, away):
            copy.start()

    half_copies = [
        remote(gate_other, gate_weights.at[own_depth, :], half_send.at[0], half_recv.at[0], {"fs": beside_x}),
        remote(project_other, project_full.at[:, own_depth], half_send.at[1], half_recv.at[1], {"fs": beside_x}),
    ]

    swap_to = (beside_x, beside_z, corner)
    swap_part = (2 * zl + 1 - x, 2 * (1 - zl) + x, 2 * (1 - zl) + 1 - x)

    def swap(a, k):
        theirs = span(swap_part[k] * units, units)
        src = up_own.at[:, theirs] if a == 0 else down_own.at[theirs, :]
        dst = up_full.at[own_depth, :] if a == 0 else down_full.at[:, own_depth]
        return remote(src, dst, swap_send.at[a, k], swap_recv.at[a, k], {"fs": swap_to[k]})

    def ff_ref(a, q, yy):
        return up_full.at[slab_at(q, yy), :] if a == 0 else down_full.at[:, slab_at(q, yy)]

    def line_of(g, b):
        return 2 * (zh if g == 0 else 1 - zh) + b

    def across(a, b):
        ref = ff_ref(a, line_of(0, b), y)
        return remote(ref, ref, across_send.at[a, b], across_recv.at[a, b], {"fs": far_z})

    def beside(a, g, b):
        ref = ff_ref(a, line_of(g, b), y)
        return remote(ref, ref, beside_send.at[a, g, b], beside_recv.at[a, g, b], {"fs": beside_y})

    def relay_gate(d, away):
        for side, step in ((0, 1), (1, -1)):
            q = z - step * d

            @pl.when((q >= 0) & (q < LINES))
            def _(q=q, side=side, step=step):
                for copy in gate_line(q, side, step, away):
                    copy.wait_recv()

                @pl.when((z + step >= 0) & (z + step < LINES))
                def _():
                    for copy in gate_line(q, side, step, away):
                        copy.start()

                for copy in gate_cross(q, y, away):
                    copy.start()

    for copy in half_copies:
        copy.start()
    start_gate(0)
    token_pair = remote(tokens_ref, token_rows.at[0, :, mine], token_send.at[0], token_recv.at[0], pair)
    token_pair.start()
    for load in loads[5:]:
        load.wait()

    @pl.loop(0, up_own.shape[1] // units)
    def _(j):
        up_own[:, span(j * units, units)] = up_ref[:, span(j * units, units)].astype(bf16)

    quarter = span((2 * zl + x) * units, units)
    swap(0, 0).start()
    token_cross = remote(
        tokens_ref, token_rows.at[1, :, mine], token_send.at[1], token_recv.at[1], {"fs": beside_x}
    )
    token_cross.start()
    up_full[own_depth, :] = up_ref[:, quarter].astype(bf16)

    @pl.loop(0, up_own.shape[1] // units)
    def _(j):
        down_own[span(j * units, units), :] = (
            down_ref[span(j * units, units), :] * down_scale_ref[...]
        ).astype(bf16)

    down_full[:, own_depth] = (down_ref[quarter, :] * down_scale_ref[...]).astype(bf16)

    for copy in half_copies:
        copy.wait_recv()
    start_gate(1)

    @pl.when(jnp.logical_not(inner))
    def _():
        swap(0, 1).start()
        swap(0, 2).start()

    def normalize(source, gain_ref, target, first, count):
        @pl.loop(0, count // fine)
        def _(i):
            these = span(first + i * fine, fine, fine)
            values = source[these, :].astype(f32)
            scaled = values * lax.rsqrt(jnp.mean(values * values, axis=-1, keepdims=True) + EPSILON)
            target[these, :] = (scaled * gain_ref[...]).astype(bf16)

    token_pair.wait()
    normalize(token_rows.at[0], mixer_gain_ref, normed.at[0], 0, rows)
    relay_gate(1, 0)
    relay_gate(1, 1)
    swap(0, 0).wait_recv()
    relay_gate(2, 0)
    relay_gate(2, 1)

    @pl.when(inner)
    def _():
        swap(0, 1).start()
        swap(0, 2).start()

    @pl.when(jnp.logical_not(inner))
    def _():
        across(0, zl).start()

    swap(1, 0).start()
    relay_gate(3, 0)
    relay_gate(3, 1)
    beside(0, 0, zl).start()
    token_cross.wait()

    @pl.when(inner)
    def _():
        across(0, zl).start()


    token_forward = remote(
        token_rows.at[1, :, mine], token_rows.at[1, :, mine], token_send.at[2], token_recv.at[2], pair
    )
    token_forward.start()
    token_forward.wait()
    normalize(token_rows.at[1], mixer_gain_ref, normed.at[1], 0, rows)

    def finish_up_swap():
        swap(0, 1).wait_recv()
        swap(0, 2).wait_recv()
        across(0, 1 - zl).start()
        beside(0, 0, 1 - zl).start()

    @pl.when(inner)
    def _():
        finish_up_swap()

    swap(1, 1).start()
    swap(1, 2).start()
    swap(1, 0).wait_recv()

    @pl.when(jnp.logical_not(inner))
    def _():
        across(1, zl).start()

    beside(1, 0, zl).start()

    def finish_down_swap():
        swap(1, 1).wait_recv()
        swap(1, 2).wait_recv()
        across(1, 1 - zl).start()

    for q in range(LINES):
        for away in range(2):
            for copy in gate_cross(q, 1 - y, away):
                copy.wait_recv()

    @pl.loop(0, 2)
    def _(s):
        linear = jnp.dot(normed[s], gate_weights[:, pl.ds(share_width, share_width)], preferred_element_type=f32)
        spatial_buf[s] = jax.nn.gelu(linear * spatial_scale_ref[:, own_channels])

    sums[...] = jnp.zeros_like(sums)
    for s in range(2):
        for n in range(blocks):
            values = spatial_buf[s, pl.ds(n * block_size, block_size), :]
            total = jnp.sum(values * values, axis=1, keepdims=True)
            sums[pl.ds(s * blocks + n, 1), :] = jnp.broadcast_to(total, (block_size, block_size)).T[:1, :]
    sum_to = (pair, {"fs": beside_x}, {"fs": beside_x, "tp": other})
    sum_copies = [remote(sums, sums_in.at[k], sum_send.at[k], sum_recv.at[k], sum_to[k]) for k in range(3)]
    for copy in sum_copies:
        copy.start()

    @pl.loop(0, 2)
    def _(s):
        linear = jnp.dot(normed[s], gate_weights[:, pl.ds(0, share_width)], preferred_element_type=f32)
        content_buf[s] = jax.nn.gelu(linear * content_scale_ref[:, own_channels])

    for copy in sum_copies:
        copy.wait_recv()

    causal = lax.broadcasted_iota(jnp.int32, (block_size, block_size), 0) >= lax.broadcasted_iota(
        jnp.int32, (block_size, block_size), 1
    )
    own_groups = groups // 2
    group_width = channels // groups
    part_copies = [
        remote(
            part.at[s, :, span(other * half, half)], part_in.at[s], part_send.at[s], part_recv.at[s], pair
        )
        for s in range(2)
    ]
    for s in (1, 0):
        for n in range(blocks):
            these = pl.ds(n * block_size, block_size)
            here, there = pl.ds(s * blocks + n, 1), pl.ds((1 - s) * blocks + n, 1)
            total = (sums[here, :] + sums_in[0, here, :]) + (sums_in[1, there, :] + sums_in[2, there, :])
            scale = lax.rsqrt(total / (2 * channels) + EPSILON)
            scale = jnp.broadcast_to(scale, (block_size, block_size)).T[:, :1]
            for g in range(own_groups):
                group = x * own_groups + g
                weights = jnp.where(causal, mixing_ref[group].astype(f32), 0.0).astype(bf16)
                bias = jnp.broadcast_to(bias_ref[pl.ds(group, 1), :], (block_size, block_size)).T[:, :1]
                at = pl.ds(g * group_width, group_width)
                gain = spatial_gain_ref[:, span(group * group_width, group_width)]
                spatial_norm = (spatial_buf[s, these, at] * scale * gain).astype(bf16)
                mixed = jnp.dot(weights, spatial_norm, preferred_element_type=f32) + bias
                gated[s, these, at] = (content_buf[s, these, at] * mixed).astype(bf16)

        @pl.loop(0, width // (2 * tile))
        def _(j, s=s):
            at = span(j * 2 * tile, 2 * tile)
            part[s, :, at] = jnp.dot(gated[s], project_full[:, at], preferred_element_type=f32).astype(bf16)

        part_copies[s].start()

    def step_rows(i):
        return pl.ds(i * block_size, block_size)

    share_copies = [
        remote(
            share.at[step_rows(i), :], share_in.at[step_rows(i), :], share_send.at[i], share_recv.at[i],
            {"fs": beside_x},
        )
        for i in range(steps)
    ]
    part_copies[1].wait_recv()
    for i in range(steps):
        these = step_rows(i)
        share[these, :] = (part[1, these, mine].astype(f32) + part_in[1, these, :].astype(f32)).astype(bf16)
        share_copies[i].start()
    part_copies[0].wait_recv()

    middle_copies = [
        remote(
            middle.at[step_rows(i), mine], middle.at[step_rows(i), mine], middle_send.at[i], middle_recv.at[i], pair
        )
        for i in range(steps)
    ]

    def row_copy(k, i):
        src = rows_all.at[2 if k == 2 else 0, step_rows(i), mine]
        dst = rows_all.at[k + 1, step_rows(i), mine]
        return remote(src, dst, row_send.at[k, i], row_recv.at[k, i], {"fs": beside_z if k == 1 else beside_x})

    def forward(k, i):
        ref = rows_all.at[k + 1, step_rows(i), mine]
        return remote(ref, ref, fwd_send.at[k, i], fwd_recv.at[k, i], pair)

    @pl.when(jnp.logical_not(inner))
    def _():
        finish_up_swap()

    for i in range(steps):
        these = step_rows(i)
        share_copies[i].wait_recv()
        total = part[0, these, mine].astype(f32) + part_in[0, these, :].astype(f32)
        total = total + share_in[these, :].astype(f32)
        middle[these, mine] = (tokens_ref[these, :].astype(f32) + total).astype(bf16)
        middle_copies[i].start()
        middle_copies[i].wait_recv()
        normalize(middle, channel_gain_ref, rows_all.at[0], i * block_size, block_size)
        row_copy(1, i).start()
        row_copy(0, i).start()
        if i == steps - 2:
            across(0, zl).wait_recv()
            beside(0, 1, zl).start()

    def pass_on(a, b):
        across(a, b).wait_recv()
        beside(a, 1, b).start()

    @pl.when(jnp.logical_not(inner))
    def _():
        pass_on(0, 1 - zl)

    for i in range(steps):
        row_copy(1, i).wait_recv()
        row_copy(2, i).start()
        forward(1, i).start()
        if i == 0:

            @pl.when(jnp.logical_not(inner))
            def _():
                finish_down_swap()

            @pl.when(inner)
            def _():
                pass_on(0, 1 - zl)

        if i == steps - 2:

            @pl.when(inner)
            def _():
                across(1, zl).start()

    @pl.when(inner)
    def _():
        finish_down_swap()

    beside(1, 0, 1 - zl).start()

    @pl.when(inner)
    def _():
        pass_on(1, zl)

    for i in range(steps):
        row_copy(0, i).wait_recv()
        forward(0, i).start()
    for g in range(2):
        for b in range(2):
            beside(0, g, b).wait_recv()

    up_tile = sizes["up_tile"]
    unit_base = (2 * zl + x) * units

    def up_product(r):
        @pl.loop(0, units // up_tile)
        def _(j):
            at = span(j * up_tile, up_tile)
            linear = jnp.dot(rows_all[r], up_full[:, at], preferred_element_type=f32)
            linear = linear * up_scale_ref[:, span(unit_base + j * up_tile, up_tile)]
            hidden[r, :, at] = jnp.square(jnp.maximum(linear, 0.0)).astype(bf16)

    up_product(0)
    for k in range(2):
        for i in range(steps):
            forward(k, i).wait_recv()
        up_product(k + 1)

    @pl.when(jnp.logical_not(inner))
    def _():
        pass_on(1, zl)

    @pl.when(inner)
    def _():
        pass_on(1, 1 - zl)


    pieces = [(g, same, late) for g in range(2) for same in range(2) for late in range(2)]

    def bit(i):
        g, same, late = pieces[i]
        if g == 0 or same == 0:
            return late
        return zl if late == 0 else 1 - zl

    def place(i):
        g, same, _ = pieces[i]
        n = 2 * same + bit(i)
        return 4 * g + n, n

    def columns(i):
        g, same, _ = pieces[i]
        return line_of(g, bit(i)), y if same == 0 else 1 - y

    def owner(i):
        return (zh if pieces[i][0] == 0 else 1 - zh) == core

    def term_copy(i, k):
        at, n = place(i)
        src, dst = (terms.at[at, 3], terms_in.at[n, 3]) if k else (terms.at[at, 0:3], terms_in.at[n, 0:3])
        return remote(src, dst, term_send.at[n, k], term_recv.at[n, k], pair)

    def routes(i):
        return (2, beside_z, 1, beside_x) if i in (3, 4, 5) else (1, beside_x, 2, beside_z)

    def cross_copy(i, k):
        at, n = place(i)
        slot, to, _, _ = routes(i)
        src = terms.at[at, 3 if k else slot]
        return remote(src, cross_in.at[n, k], cross_send.at[n, k], cross_recv.at[n, k], {"fs": to})

    def line_copy(i):
        at, n = place(i)
        _, _, slot, to = routes(i)
        return remote(terms.at[at, slot], line_in.at[n], line_send.at[n], line_recv.at[n], {"fs": to})

    arrived = set()

    def product_step(i, k):
        g, same, _ = pieces[i]
        if same == 1 and i not in arrived:
            beside(1, g, bit(i)).wait_recv()
        arrived.add(i)
        at, _ = place(i)
        q, yy = columns(i)

        def product(r):
            terms[at, r] = jnp.dot(hidden[r], down_full[:, slab_at(q, yy)], preferred_element_type=f32).astype(bf16)

        if k == 0:
            pl.loop(0, 3)(product)
        else:
            product(3)

        @pl.when(jnp.logical_not(owner(i)))
        def _():
            term_copy(i, k).start()

    def add_step(i, k):
        at, n = place(i)

        @pl.when(owner(i))
        def _():
            term_copy(i, k).wait_recv()

            def add(r):
                @pl.loop(0, rows // fine)
                def _(c):
                    these = span(c * fine, fine, fine)
                    terms[at, r, these, :] = (
                        terms[at, r, these, :].astype(f32) + terms_in[n, r, these, :].astype(f32)
                    ).astype(bf16)

            first, _, second, _ = routes(i)
            if k == 1:
                add(3)
                cross_copy(i, 1).start()
            else:
                add(first)
                cross_copy(i, 0).start()
                add(second)
                add(0)

    def cross_step(i):
        at, n = place(i)

        @pl.when(owner(i))
        def _():
            cross_copy(i, 1).wait_recv()
            slot = routes(i)[2]

            @pl.loop(0, rows // fine)
            def _(c):
                these = span(c * fine, fine, fine)
                terms[at, slot, these, :] = (
                    terms[at, slot, these, :].astype(f32) + cross_in[n, 1, these, :].astype(f32)
                ).astype(bf16)

            line_copy(i).start()
            cross_copy(i, 0).wait_recv()

    def out_copy(i):
        q, yy = columns(i)
        cols = slab_at(q % 2, yy)
        return pltpu.make_async_copy(out_ref.at[:, cols], out_hbm.at[:, cols], out_sem.at[place(i)[1]])

    def line_step(i):
        at, n = place(i)
        q, yy = columns(i)

        @pl.when(owner(i))
        def _():
            line_copy(i).wait_recv()
            out_at = slab_at(q % 2, yy)

            @pl.loop(0, rows // fine)
            def _(c):
                these = span(c * fine, fine, fine)
                total = terms[at, 0, these, :].astype(f32) + cross_in[n, 0, these, :].astype(f32)
                total = total + line_in[n, these, :].astype(f32)
                out_ref[these, out_at] = (middle[these, slab_at(q, yy)].astype(f32) + total).astype(bf16)

            out_copy(i).start()

    def far_step(i):
        @pl.when(jnp.logical_not(inner))
        def _():
            pass_on(1, 1 - zl)

    def run_tail(names):
        kinds = dict(
            p=lambda i: (product_step(i, 1), product_step(i, 0)),
            q=lambda i: product_step(i, 0),
            r=lambda i: product_step(i, 1),
            a=lambda i: (add_step(i, 1), add_step(i, 0)),
            b=lambda i: add_step(i, 0),
            d=lambda i: add_step(i, 1),
            c=cross_step,
            l=line_step,
            f=far_step,
        )
        for name in names:
            kinds[name[0]](int(name[1]))

    run_tail(sizes["early"])
    for i in range(steps):
        row_copy(2, i).wait_recv()
        forward(2, i).start()
    for i in range(steps):
        forward(2, i).wait_recv()
    up_product(3)
    run_tail(sizes["late"])

    for copy in half_copies + sum_copies + part_copies + share_copies + middle_copies:
        copy.wait_send()
    for a in range(2):
        for k in range(3):
            swap(a, k).wait_send()
        for b in range(2):
            across(a, b).wait_send()
            for g in range(2):
                beside(a, g, b).wait_send()
    for q in range(LINES):
        for away in range(2):
            for copy in gate_cross(q, y, away):
                copy.wait_send()
    for side, step in ((0, 1), (1, -1)):
        for d in range(LINES):
            q = z - step * d

            @pl.when((q >= 0) & (q < LINES) & (z + step >= 0) & (z + step < LINES))
            def _(q=q, side=side, step=step):
                for away in range(2):
                    for copy in gate_line(q, side, step, away):
                        copy.wait_send()

    for k in range(3):
        for i in range(steps):
            row_copy(k, i).wait_send()
            forward(k, i).wait_send()
    for i in range(8):

        @pl.when(owner(i))
        def _(i=i):
            out_copy(i).wait()

    for i in range(4):
        for k in range(2):
            cross_copy(i, k).wait_send()
        line_copy(i).wait_send()
        for k in range(2):
            term_copy(i, k).wait_send()


def fused_shards(fs, tokens, mixer_gain, w_content, w_spatial, content_scale, spatial_scale, spatial_gain,
                 block_mixing, block_bias, w_project, project_scale, channel_gain, w_up, up_scale, w_down, down_scale):
    rows, half = tokens.shape
    width = 2 * half
    channels = w_content.shape[1]
    share_width = channels // 2
    hidden_units = w_up.shape[1]
    units = hidden_units // 4
    depth = w_up.shape[0]
    slab = 2 * depth
    steps = rows // block_mixing.shape[1]
    bf16, f32 = jnp.bfloat16, jnp.float32
    early = [
        "q0", "q2", "b0", "b2",
    ]
    late = [
        "r0", "r2", "d0", "f1", "p4", "d2", "p5", "a4", "p1", "a5", "p6", "a1", "p3", "a6", "c0", "a3", "c2",
        "p7", "a7", "c4", "c5", "c1", "c6", "c3", "c7", "l0", "l2", "l4", "l5", "l1", "l3", "l6", "l7",
    ]
    sizes = dict(fine=128, tile=256, up_tile=256, early=early, late=late)
    vmem = pltpu.VMEM
    dma = pltpu.SemaphoreType.DMA
    row = lambda a: a.reshape(1, -1)
    operands = (
        tokens, row(mixer_gain), w_content, w_spatial, row(content_scale), row(spatial_scale), row(spatial_gain),
        block_mixing, block_bias, w_project, row(project_scale), row(channel_gain), w_up, row(up_scale), w_down,
        row(down_scale),
    )
    sems = [(3,), (2,), None, None, (2, 3), (2, 2), (2, 2, 2), (3,), (2,), (steps,), (steps,), (3, steps), (3, steps),
            (4, 2), (4, 2), (4,)]
    pairs = []
    for shape in sems:
        if shape is not None:
            pairs += [dma(shape), dma(shape)]
        elif len(pairs) == 4:
            pairs += [dma((2, 2, 2, LINES)), dma((2, 2, LINES))]
        else:
            pairs += [dma((2, 2, LINES)), dma((2, 2, LINES))]
    return pl.pallas_call(
        functools.partial(layer_kernel, sizes),
        out_shape=jax.ShapeDtypeStruct((rows, half), bf16),
        in_specs=[
            pl.BlockSpec(memory_space=pl.ANY) for _ in range(16)
        ],
        out_specs=pl.BlockSpec(memory_space=pl.ANY),
        scratch_shapes=[
            *[vmem(a.shape, a.dtype) for a in operands],
            dma((len(operands),)),
            vmem((2, rows, width), bf16),
            vmem((2, rows, width), bf16),
            vmem((width, 2 * share_width), bf16),
            vmem((share_width, width), bf16),
            vmem((depth, 2 * share_width), bf16),
            vmem((share_width, depth), bf16),
            vmem((depth, hidden_units), bf16),
            vmem((hidden_units, depth), bf16),
            vmem((width, units), bf16),
            vmem((units, width), bf16),
            vmem((2, rows, share_width), f32),
            vmem((2, rows, share_width), f32),
            vmem((2, rows, share_width), bf16),
            vmem((8, 128), f32),
            vmem((3, 8, 128), f32),
            vmem((2, rows, width), bf16),
            vmem((2, rows, half), bf16),
            vmem((rows, half), bf16),
            vmem((rows, half), bf16),
            vmem((rows, width), bf16),
            vmem((4, rows, width), bf16),
            vmem((4, rows, units), bf16),
            vmem((8, 4, rows, slab), bf16),
            vmem((4, 4, rows, slab), bf16),
            vmem((4, 2, rows, slab), bf16),
            vmem((4, rows, slab), bf16),
        ] + pairs + [vmem((rows, half), bf16), dma((4,))],
        compiler_params=pltpu.CompilerParams(
            collective_id=0, has_side_effects=True, vmem_limit_bytes=VMEM_LIMIT
        ),
    )(*operands)


VMEM_LIMIT = 67043328


def solution(mesh):
    fs, tp = mesh.shape["fs"], mesh.shape["tp"]
    if tp == 2 and fs == LINES * PLANE:
        body = functools.partial(fused_shards, fs)
    else:
        body = shards
    return jax.shard_map(
        body,
        mesh=mesh,
        in_specs=(
            P("fs", "tp"),
            P(),
            P("fs", "tp"),
            P("fs", "tp"),
            P("tp"),
            P("tp"),
            P("tp"),
            P("tp", None, None),
            P("tp", None),
            P("tp", "fs"),
            P("fs"),
            P(),
            P("fs", "tp"),
            P("tp"),
            P("tp", "fs"),
            P("fs"),
        ),
        out_specs=P("fs", "tp"),
        check_vma=False,
    )
```
